256 devices in a mesh: tp: 32 (over z, y), dp: 8 (over x, core).
Axes of the slice: x: 4, y: 4, z: 8, core: 2. Of those that a mesh axis runs over, the one named last changes fastest.
Arguments:
- tokens: bfloat16 [128, 16, 4096], P('tp', None, 'dp'), may hold values from -24 to 24
- lengths: int32 [128], P('dp'), may hold values from 1 to 16, 896 in all
- norm_gain: float32 [2, 4096], P(None, 'dp'), may hold values from 0.1 to 1.9
- query_weight: bfloat16 [2, 4096, 4096], P(None, 'dp', 'tp'), may hold values from -0.09375 to 0.09375
- key_weight: bfloat16 [2, 4096, 4096], P(None, 'dp', 'tp'), may hold values from -0.09375 to 0.09375
- value_weight: bfloat16 [2, 4096, 4096], P(None, 'dp', 'tp'), may hold values from -0.09375 to 0.09375
- outgate_weight: bfloat16 [2, 4096, 4096], P(None, 'dp', 'tp'), may hold values from -0.09375 to 0.09375
- input_gate_weight: bfloat16 [2, 4096, 32], replicated, may hold values from -0.09375 to 0.09375
- forget_gate_weight: bfloat16 [2, 4096, 32], replicated, may hold values from -0.09375 to 0.09375
- forget_bias: float32 [2, 32], P(None, 'tp'), may hold values from -1 to 6
- out_weight: bfloat16 [2, 4096, 4096], P(None, 'tp', 'dp'), may hold values from -0.09375 to 0.09375
- cell_state: float32 [2, 128, 32, 128, 128], P(None, 'dp', 'tp'), may hold values from -1.5 to 1.5
- norm_state: float32 [2, 128, 32, 128], P(None, 'dp', 'tp'), may hold values from -1.5 to 1.5
- max_state: float32 [2, 128, 32], P(None, 'dp', 'tp'), may hold values from -6 to 6
Outputs:
- tokens_next: bfloat16 [128, 16, 4096], P('tp', None, 'dp')
- cell_next: float32 [2, 128, 32, 128, 128], P(None, 'dp', 'tp')
- norm_next: float32 [2, 128, 32, 128], P(None, 'dp', 'tp')
- max_next: float32 [2, 128, 32], P(None, 'dp', 'tp')
The draws below stay inside these ranges and needn't reach their ends.
Inputs may be any that keep to these rules, and one draw needn't show every extreme that they name: `lengths`: the largest is 16.
All inputs are finite; a program needn't handle non-finite values. No bound on the sum of `lengths` on one device may be relied on, other than what follows from the above.
Results may differ from the reference program's by a relative error of at most 0.025.
Values may be sent and summed in bfloat16 or wider, within the bound.
No kernel may reach another device: no remote copies, remote signals or barrier semaphores. Data moves between devices by JAX's collectives and lax.ppermute only.
A program may use at most 64 MiB of HBM per device.

```python
import math
import jax
import jax.numpy as jnp
import numpy as np
from jax import lax

D = 4096
HEADS = 32
HEAD_DIM = 128
STEP = 16
SEQS = 128
W = 4096
N_DP = 8


def draw_tokens(key, part):
    first = jax.random.fold_in(jax.random.fold_in(key, 11), 0)
    position = jnp.arange(D, dtype=jnp.float32) / D
    noise = jnp.clip(jax.random.normal(first, (SEQS, STEP, D), jnp.float32), -4.0, 4.0)
    ramp_scale = 0.5 * jnp.exp(jnp.log(4.0) * position)
    return (noise * ramp_scale).astype(jnp.bfloat16)


def shard_levels(stream_key, shape, shards, low, high):
    def one(axis_at, parts):
        draws = jax.random.uniform(jax.random.fold_in(jax.random.fold_in(stream_key, 6), axis_at), (parts,), jnp.float32, low / len(shards), high / len(shards))
        return jnp.repeat(jnp.exp(draws), shape[axis_at] // parts).reshape((-1,) + (1,) * (len(shape) - axis_at - 1))

    level = one(*shards[0])
    for cut in shards[1:]:
        level = level * one(*cut)
    return level


def profile(count, total, most, skew):
    loads = [(1 << 20) // math.isqrt(standing ** skew) + 1 for standing in range(2, count + 1)]
    surplus, holding = total - most - (count - 1), [1] * (count - 1)
    while surplus > 0:
        candidates = [i for i in range(count - 1) if holding[i] < most]
        whole, remaining = sum([loads[i] for i in candidates]), surplus
        for i in candidates:
            extra = min(most - holding[i], max(1, remaining * loads[i] // whole), surplus)
            holding[i] = holding[i] + extra
            surplus = surplus - extra
    return np.array([most] + holding)


def ragged_sizes(stream_key, count, total, reach, slope):
    if count == 2:
        one = jax.random.randint(stream_key, (), max(1, total - reach), min(reach, total - 1) + 1)
        return jnp.stack([one, total - one])
    sizes = jnp.asarray(profile(count, total, reach, slope), jnp.int32)
    twos = (count - 1) // 2
    donor, taker = sizes[1:1 + 2 * twos:2], sizes[2:2 + 2 * twos:2]
    margin = jnp.minimum(donor - 1, reach - taker)
    passed = jax.random.randint(jax.random.fold_in(stream_key, 1), (twos,), 0, 1 << 20) % (margin + 1)
    sizes = sizes.at[1:1 + 2 * twos:2].set(donor - passed).at[2:2 + 2 * twos:2].set(taker + passed)
    return sizes[jax.random.permutation(jax.random.fold_in(stream_key, 2), count)]


def bell_draw(stream_key, extent, scale, reach, cuts=(), kind=jnp.bfloat16):
    array = scale * jax.random.normal(stream_key, extent, jnp.float32)
    if cuts:
        array = array * shard_levels(stream_key, extent, cuts, -0.22, 0.18)
    return jnp.clip(array, -reach, reach).astype(kind)


def setup_inputs(seed: int = 0) -> dict:
    key_of = jax.random.split(jax.random.key(seed), 15)
    return {
        "tokens": draw_tokens(jax.random.fold_in(key_of[14], 71), 0),
        "lengths": ragged_sizes(key_of[1], SEQS, SEQS * 7, STEP, 2).astype(jnp.int32),
        "norm_gain": jnp.clip(1.0 + 0.18 * jax.random.normal(key_of[2], (2, D), jnp.float32), 0.1, 1.9),
        "query_weight": bell_draw(key_of[3], (2, D, W), D ** -0.5, 0.09375, ((1, 8), (2, 32))),
        "key_weight": bell_draw(key_of[4], (2, D, W), D ** -0.5, 0.09375, ((1, 8), (2, 32))),
        "value_weight": bell_draw(key_of[5], (2, D, W), D ** -0.5, 0.09375, ((1, 8), (2, 32))),
        "outgate_weight": bell_draw(key_of[6], (2, D, W), D ** -0.5, 0.09375, ((1, 8), (2, 32))),
        "input_gate_weight": bell_draw(key_of[7], (2, D, HEADS), D ** -0.5, 0.09375),
        "forget_gate_weight": bell_draw(key_of[8], (2, D, HEADS), D ** -0.5, 0.09375),
        "forget_bias": jnp.clip(-1.0 + 7.0 * jax.random.uniform(key_of[9], (2, HEADS), jnp.float32) ** shard_levels(key_of[9], (2, HEADS), ((1, 32),), -0.2, 0.2), -1.0, 6.0),
        "out_weight": bell_draw(key_of[10], (2, W, D), W ** -0.5, 0.09375, ((1, 32), (2, 8))),
        "cell_state": bell_draw(key_of[11], (2, SEQS, HEADS, HEAD_DIM, HEAD_DIM), 0.25, 1.5, ((1, 8), (2, 32)), jnp.float32),
        "norm_state": bell_draw(key_of[12], (2, SEQS, HEADS, HEAD_DIM), 0.25, 1.5, ((1, 8), (2, 32)), jnp.float32),
        "max_state": bell_draw(key_of[13], (2, SEQS, HEADS), 1.0, 6.0, ((1, 8), (2, 32)), jnp.float32),
    }


EPSILON = 1e-06
NEG_FILL = -1e+30

def cell_update(cell, normer, stabil, query, key_vec, value, in_gate, log_forget, live):
    high = lax.Precision.HIGHEST
    in_gate = jnp.where(live, in_gate, NEG_FILL)
    log_forget = jnp.where(live, log_forget, 0.0)
    cumul = jnp.cumsum(log_forget, axis=-1)
    span = query.shape[2]
    causal = jnp.tril(jnp.ones((span, span), dtype=bool))
    log_weight = jnp.where(causal, cumul[..., :, None] - cumul[..., None, :] + in_gate[..., None, :], NEG_FILL)
    carried = cumul + stabil[..., None]
    running = jnp.maximum(lax.optimization_barrier(jnp.max(log_weight, axis=-1)), carried)
    carry_scale = jnp.exp(carried - running)
    scores = jnp.einsum('bhtd,bhud->bhtu', query, key_vec, precision=high) * jnp.exp(log_weight - running[..., None])
    numer = jnp.einsum('bhtu,bhue->bhte', scores, value, precision=high)
    numer = numer + carry_scale[..., None] * jnp.einsum('bhtd,bhde->bhte', query, cell, precision=high)
    denom = lax.optimization_barrier(jnp.sum(scores, axis=-1)) + carry_scale * jnp.einsum('bhtd,bhd->bht', query, normer, precision=high)
    readout = numer / jnp.maximum(jnp.abs(denom), 1.0)[..., None]
    readout = jnp.where(live[..., None], readout, 0.0)
    stabil_next = running[..., -1]
    source_weight = jnp.exp(cumul[..., -1:] - cumul + in_gate - stabil_next[..., None])
    decay = jnp.exp(cumul[..., -1] + stabil - stabil_next)
    cell_next = decay[..., None, None] * cell + jnp.einsum('bhu,bhud,bhue->bhde', source_weight, key_vec, value, precision=high)
    normer_next = decay[..., None] * normer + jnp.einsum('bhu,bhud->bhd', source_weight, key_vec, precision=high)
    return (cell_next, normer_next, stabil_next, readout)

def summed_blocks(scaled, weight, pieces):
    rows_each = scaled.shape[1] // pieces
    total = jnp.zeros((scaled.shape[0], weight.shape[1]), jnp.float32)
    for piece_index in range(pieces):
        lower = piece_index * rows_each
        part = jnp.dot(scaled[:, lower:lower + rows_each], weight[lower:lower + rows_each], preferred_element_type=jnp.float32)
        total = total + lax.optimization_barrier(part.astype(jnp.bfloat16)).astype(jnp.float32)
    return total

def to_heads(flat, seqs, span, heads):
    return jnp.transpose(flat.reshape(seqs, span, heads, -1), (0, 2, 1, 3)).astype(jnp.float32)

def reference(tokens, lengths, norm_gain, query_weight, key_weight, value_weight, outgate_weight, input_gate_weight, forget_gate_weight, forget_bias, out_weight, cell_state, norm_state, max_state):
    seqs, span, width = tokens.shape
    heads = cell_state.shape[2]
    head_size = cell_state.shape[3]
    live = (jnp.arange(span, dtype=jnp.int32)[None, :] < lengths[:, None])[:, None, :]
    current = tokens
    cells, normers, stabils = ([], [], [])
    for layer_index in range(2):
        flat = current.reshape(seqs * span, width)
        widened = flat.astype(jnp.float32)
        scale = lax.rsqrt(lax.optimization_barrier(jnp.mean(widened * widened, axis=-1, keepdims=True)) + EPSILON)
        scaled = (widened * norm_gain[layer_index]).astype(jnp.bfloat16)

        def project(weight):
            return (scale * summed_blocks(scaled, weight, N_DP)).astype(jnp.bfloat16)
        query = to_heads(project(query_weight[layer_index]), seqs, span, heads)
        key_vec = to_heads(project(key_weight[layer_index]), seqs, span, heads) * head_size ** (-0.5)
        value = to_heads(project(value_weight[layer_index]), seqs, span, heads)
        outgate = project(outgate_weight[layer_index]).astype(jnp.float32)
        gate_weights = jnp.concatenate([input_gate_weight[layer_index], forget_gate_weight[layer_index]], axis=1)
        gate_both = scale * summed_blocks(scaled, gate_weights, N_DP)
        in_gate = jnp.transpose(gate_both[:, :heads].reshape(seqs, span, heads), (0, 2, 1))
        log_forget = jax.nn.log_sigmoid(jnp.transpose(gate_both[:, heads:].reshape(seqs, span, heads) + forget_bias[layer_index], (0, 2, 1)))
        cell_next, normer_next, stabil_next, readout = cell_update(cell_state[layer_index], norm_state[layer_index], max_state[layer_index], query, key_vec, value, in_gate, log_forget, live)
        cells.append(cell_next)
        normers.append(normer_next)
        stabils.append(stabil_next)
        readout = jnp.transpose(readout, (0, 2, 1, 3)).reshape(seqs * span, heads * head_size)
        gated = (readout * jax.nn.sigmoid(outgate)).astype(jnp.bfloat16)
        mixed = jnp.dot(gated, out_weight[layer_index], preferred_element_type=jnp.float32)
        current = (widened + mixed).astype(jnp.bfloat16).reshape(seqs, span, width)
    return (current, jnp.stack(cells), jnp.stack(normers), jnp.stack(stabils))
```

```python
import jax
import jax.numpy as jnp
from jax import lax
from jax.experimental import pallas as pl
from jax.experimental.pallas import tpu as pltpu
from jax.sharding import Mesh
from jax.sharding import PartitionSpec as P

TP = ("zh", "zl", "y")
DP = ("x", "c")
ZZ = ("zl", "zh")
YX = ("y", "x")

EPSILON = 1e-06
NEG_FILL = -1e30
F32 = jnp.float32
BF16 = jnp.bfloat16
EXTRA = 8


def split_pair(value):
    high = value.astype(BF16)
    return high, (value - high.astype(F32)).astype(BF16)


def dot(a, b):
    return lax.dot_general(a, b, (((1,), (0,)), ((), ())), preferred_element_type=F32)


def dot_nt(a, b):
    return lax.dot_general(a, b, (((1,), (1,)), ((), ())), preferred_element_type=F32)


def project_kernel(where, tokens, gain, gates, *rest):
    weights, out = rest[:-1], rest[-1]
    y, c = where[0], where[1]
    ny = len(weights) // 2
    nx, toks, feat = tokens.shape[1:]
    halves = []
    squares = []
    for half in (c, 1 - c):
        wide = tokens[half].reshape(nx * toks, feat).astype(F32)
        halves.append((wide * gain[pl.ds(half, 1), :]).astype(BF16))
        squares.append(split_pair(wide * wide))
    gate_half = [gates[c], gates[1 - c]]
    ones = jnp.ones((8, feat), BF16)
    extras = []
    for xi in range(nx):
        rows = slice(xi * toks, (xi + 1) * toks)
        both = dot_nt(gate_half[0], halves[0][rows]) + dot_nt(gate_half[1], halves[1][rows])
        square = sum(dot_nt(ones, part[rows]) for pair in squares for part in pair)
        extras.append((both, square))
    for k in range(ny):
        head = lax.rem(y + ny - k, ny)
        done = dot(halves[0], weights[2 * k][...]) + dot(halves[1], weights[2 * k + 1][...])
        out[head, :, :toks, :] = done.astype(BF16).reshape(nx, toks, done.shape[1])
    out[:, :, toks:, :] = jnp.zeros((ny, nx, EXTRA, out.shape[3]), BF16)
    for xi in range(nx):
        both, square = extras[xi]
        high, low = (p.astype(F32) for p in split_pair(both))
        s_high, s_low = (p.astype(F32) for p in split_pair(square))
        for head in range(ny):
            a, b = 2 * head, 2 * head + 1
            block = jnp.concatenate(
                [
                    high[a : a + 1],
                    low[a : a + 1],
                    high[b : b + 1],
                    low[b : b + 1],
                    s_high[0:1],
                    s_low[0:1],
                    jnp.zeros((2, toks), F32),
                ],
                axis=0,
            )
            out[head, xi, toks:, :toks] = block.astype(BF16)


def cell_kernel(width, span, parts, aux, cell, normer, cell_out, normer_out, stabil_out, gated):
    toks = gated.shape[2]
    size = cell.shape[1]
    seqs = toks // span
    total = parts[0, 0].astype(F32)
    for xi in range(1, parts.shape[1]):
        total = total + parts[0, xi].astype(F32)
    rows = jnp.concatenate([total[toks:, :128], aux[0]], axis=0)
    cols = jnp.transpose(rows)[:toks]
    rows = rows[:, :toks]

    def small(get):
        scale = lax.rsqrt((get(4) + get(5)) / width + EPSILON)
        live = get(9) > 0.5
        gate_in = jnp.where(live, scale * (get(0) + get(1)), NEG_FILL)
        forget = scale * (get(2) + get(3)) + get(10)
        log_forget = jnp.minimum(forget, 0.0) - jnp.log1p(jnp.exp(-jnp.abs(forget)))
        return scale, live, gate_in, jnp.where(live, log_forget, 0.0), get(8)

    _, _, in_row, lf_row, m_row = small(lambda i: rows[i : i + 1])
    scale, live, in_col, lf_col, m_col = small(lambda i: cols[:, i : i + 1])
    at_row = lax.broadcasted_iota(jnp.int32, (toks, toks), 0)
    at_col = lax.broadcasted_iota(jnp.int32, (toks, toks), 1)
    same = (at_row // span) == (at_col // span)
    causal = same & (at_col <= at_row)
    anti = same & (at_row <= at_col)
    c_col = jnp.sum(jnp.where(causal, lf_row, 0.0), axis=1, keepdims=True)
    c_row = jnp.sum(jnp.where(anti, lf_col, 0.0), axis=0, keepdims=True)
    last_col = jnp.sum(jnp.where(same, lf_row, 0.0), axis=1, keepdims=True)
    last_row = jnp.sum(jnp.where(same, lf_col, 0.0), axis=0, keepdims=True)
    weight = jnp.where(causal, c_col - c_row + in_row, NEG_FILL)
    carried = c_col + m_col
    running = jnp.maximum(jnp.max(weight, axis=1, keepdims=True), carried)
    carry = jnp.exp(carried - running)

    def piece(i):
        return (scale * total[:toks, i * size : (i + 1) * size]).astype(BF16)

    query, key_vec, value, outgate = (piece(i) for i in range(4))
    shrink = size**-0.5
    scores = dot_nt(query, key_vec) * shrink * jnp.exp(weight - running)
    s_high, s_low = split_pair(scores)
    carried_out = []
    carried_norm = []
    query_wide = query.astype(F32)
    for r in range(seqs):
        at = slice(r * span, (r + 1) * span)
        high, low = split_pair(cell[r])
        carried_out.append(dot(query[at], high) + dot(query[at], low))
        carried_norm.append(jnp.sum(query_wide[at] * normer[0, r : r + 1], axis=1, keepdims=True))
    numer = dot(s_high, value) + dot(s_low, value) + carry * jnp.concatenate(carried_out, axis=0)
    denom = jnp.sum(scores, axis=1, keepdims=True) + carry * jnp.concatenate(carried_norm, axis=0)
    readout = jnp.where(live, numer / jnp.maximum(jnp.abs(denom), 1.0), 0.0)
    mixed = (readout * jax.nn.sigmoid(outgate.astype(F32))).astype(BF16)
    for xi in range(gated.shape[1]):
        gated[0, xi] = mixed

    top_col = jnp.maximum(
        jnp.max(jnp.where(same, last_col - c_row + in_row, NEG_FILL), axis=1, keepdims=True),
        last_col + m_col,
    )
    top_row = jnp.maximum(
        jnp.max(jnp.where(same, last_row - c_col + in_col, NEG_FILL), axis=0, keepdims=True),
        last_row + m_row,
    )
    source = jnp.exp(last_col - c_col + in_col - top_col)
    decay = jnp.exp(last_col + m_col - top_col)
    keyed = (key_vec.astype(F32) * shrink) * source
    k_high, k_low = split_pair(jnp.transpose(keyed))
    token_seq = lax.broadcasted_iota(jnp.int32, (toks, size), 0) // span
    for r in range(seqs):
        at = slice(r * span, (r + 1) * span)
        one = jnp.where(token_seq == r, value.astype(F32), 0.0).astype(BF16)
        fade = decay[r * span : r * span + 1]
        cell_out[r] = fade * cell[r] + (dot(k_high, one) + dot(k_low, one))
        normer_out[0, r : r + 1] = fade * normer[0, r : r + 1] + jnp.sum(
            keyed[at], axis=0, keepdims=True
        )
    stabil_out[0] = jnp.broadcast_to(top_row, (8, toks))


def mix_kernel(where, gated, *rest):
    weights, out = rest[:-1], rest[-1]
    y = where[0]
    ny = len(weights)
    cores, _, nx, toks, size = gated.shape
    for core in range(cores):
        total = None
        for k in range(ny):
            head = lax.rem(y + ny - k, ny)
            part = dot(gated[core, head].reshape(nx * toks, size), weights[k][...])
            total = part if total is None else total + part
        out[core] = total.astype(BF16).reshape(nx, toks, total.shape[1])


def add_kernel(parts, own, out, spread):
    total = parts[0].astype(F32)
    for i in range(1, parts.shape[0]):
        total = total + parts[i].astype(F32)
    done = (own[...].astype(F32) + total).astype(BF16)
    out[...] = done
    for i in range(spread.shape[0]):
        spread[i] = done


SMEM_SPEC = pl.BlockSpec(memory_space=pltpu.SMEM)
VMEM_SPEC = pl.BlockSpec(memory_space=pltpu.VMEM)


def per_device(
    tokens,
    lengths,
    norm_gain,
    query_weight,
    key_weight,
    value_weight,
    outgate_weight,
    input_gate_weight,
    forget_gate_weight,
    forget_bias,
    out_weight,
    cell_state,
    norm_state,
    max_state,
):
    seq_here, span, feat = tokens.shape
    layers, local_seqs, _, size, _ = cell_state.shape
    ny, nx, nc, nz = (lax.axis_size(a) for a in ("y", "x", "c", ZZ))
    toks = seq_here * span
    width = feat * nx * nc
    y, x, c = (lax.axis_index(a) for a in ("y", "x", "c"))
    z = lax.axis_index("zh") * lax.axis_size("zl") + lax.axis_index("zl")
    where = jnp.stack([y, c]).astype(jnp.int32)
    quarters = local_seqs // seq_here

    def shifted(array, step):
        return lax.ppermute(array, "y", [(i, (i + step) % ny) for i in range(ny)])

    def swapped(array):
        return lax.ppermute(array, "c", [(i, (i + 1) % nc) for i in range(nc)])

    def weights_of(layer):
        return jnp.concatenate(
            [w[layer] for w in (query_weight, key_weight, value_weight, outgate_weight)], axis=1
        )

    gains = lax.all_gather(norm_gain, "c", axis=0)
    live = jnp.arange(span, dtype=jnp.int32)[None, :] < lengths[:, None]

    def aux_of(layer):
        m = jnp.broadcast_to(max_state[layer], (local_seqs, span)).reshape(quarters, 1, toks)
        alive = live.astype(F32).reshape(quarters, 1, toks)
        bias = jnp.broadcast_to(forget_bias[layer, 0], (quarters, 1, toks))
        rows = jnp.concatenate([m, alive, bias, jnp.zeros((quarters, 5, toks), F32)], axis=1)
        return jnp.pad(rows, ((0, 0), (0, 0), (0, 128 - toks)))

    def gates_of(layer):
        cut = [
            lax.dynamic_slice(w[layer], (x * nc * feat, z * ny), (nc * feat, ny))
            for w in (input_gate_weight, forget_gate_weight)
        ]
        both = jnp.stack(cut, axis=2).reshape(nc, feat, 2 * ny)
        return jnp.transpose(both, (0, 2, 1))

    def gather_weights(joined):
        own = [joined] + [shifted(joined, k) for k in range(1, ny)]
        pairs = []
        for w in own:
            pairs += [w, swapped(w)]
        return pairs

    current = tokens.reshape(toks, feat)
    spread = jnp.broadcast_to(current[None], (nz, toks, feat))
    weights = gather_weights(weights_of(0))
    cells, normers, stabils = [], [], []
    for layer in range(layers):
        arrived = lax.all_to_all(spread, ZZ, 0, 0, tiled=True)
        halves = lax.all_to_all(
            arrived.reshape(nc, nx * toks, feat), "c", 0, 0, tiled=True
        ).reshape(nc, nx, toks, feat)
        parts = pl.pallas_call(
            project_kernel,
            out_shape=jax.ShapeDtypeStruct((ny, nx, toks + EXTRA, 4 * size), BF16),
            in_specs=[SMEM_SPEC] + [VMEM_SPEC] * (3 + 2 * ny),
            out_specs=VMEM_SPEC,
            name=f"project_{layer}",
        )(where, halves, gains[:, layer], gates_of(layer), *weights)
        summed = lax.all_to_all(
            parts.reshape(ny * nx, toks + EXTRA, 4 * size), YX, 0, 0, tiled=True
        ).reshape(ny, nx, toks + EXTRA, 4 * size)
        if layer == 0:
            own_out, summed = lax.optimization_barrier((out_weight[layer], summed))
            outs = [own_out] + [shifted(own_out, k) for k in range(1, ny)]
        cell_next, normer_next, top, gated = pl.pallas_call(
            lambda *refs: cell_kernel(width, span, *refs),
            grid=(quarters,),
            out_shape=(
                jax.ShapeDtypeStruct((local_seqs, size, size), F32),
                jax.ShapeDtypeStruct((quarters, seq_here, size), F32),
                jax.ShapeDtypeStruct((quarters, 8, toks), F32),
                jax.ShapeDtypeStruct((quarters, nx, toks, size), BF16),
            ),
            in_specs=[
                pl.BlockSpec((1, nx, toks + EXTRA, 4 * size), lambda i: (i, 0, 0, 0)),
                pl.BlockSpec((1, 8, 128), lambda i: (i, 0, 0)),
                pl.BlockSpec((seq_here, size, size), lambda i: (i, 0, 0)),
                pl.BlockSpec((1, seq_here, size), lambda i: (i, 0, 0)),
            ],
            out_specs=(
                pl.BlockSpec((seq_here, size, size), lambda i: (i, 0, 0)),
                pl.BlockSpec((1, seq_here, size), lambda i: (i, 0, 0)),
                pl.BlockSpec((1, 8, toks), lambda i: (i, 0, 0)),
                pl.BlockSpec((1, nx, toks, size), lambda i: (i, 0, 0, 0)),
            ),
            name=f"cell_{layer}",
        )(
            summed,
            aux_of(layer),
            cell_state[layer, :, 0],
            norm_state[layer, :, 0].reshape(quarters, seq_here, size),
        )
        cells.append(cell_next[:, None])
        normers.append(normer_next.reshape(local_seqs, 1, size))
        stabils.append(top[:, 0, ::span].reshape(local_seqs, 1))
        heads = lax.all_to_all(
            gated.reshape(quarters * nx, toks, size), YX, 0, 0, tiled=True
        ).reshape(ny, nx, toks, size)
        everyone = lax.all_gather(heads, "c", axis=0)
        mixed = pl.pallas_call(
            mix_kernel,
            out_shape=jax.ShapeDtypeStruct((nc, nx, toks, feat), BF16),
            in_specs=[SMEM_SPEC] + [VMEM_SPEC] * (1 + ny),
            out_specs=VMEM_SPEC,
            name=f"mix_{layer}",
        )(where, everyone, *outs)
        mixed = mixed.reshape(nz, toks, feat)
        if layer + 1 < layers:
            joined, mixed = lax.optimization_barrier(
                (jnp.concatenate([weights_of(layer + 1), out_weight[layer + 1]], axis=0), mixed)
            )
            moved = [joined] + [shifted(joined, k) for k in range(1, ny)]
            weights = []
            for w in moved:
                weights += [w[:feat], swapped(w[:feat])]
            outs = [w[feat:] for w in moved]
        added = lax.all_to_all(mixed, ZZ, 0, 0, tiled=True)
        current, spread = pl.pallas_call(
            add_kernel,
            out_shape=(
                jax.ShapeDtypeStruct((toks, feat), BF16),
                jax.ShapeDtypeStruct((nz, toks, feat), BF16),
            ),
            in_specs=[VMEM_SPEC] * 2,
            out_specs=(VMEM_SPEC, VMEM_SPEC),
            name=f"add_{layer}",
        )(added, current)
    return (
        current.reshape(seq_here, span, feat),
        jnp.stack(cells),
        jnp.stack(normers),
        jnp.stack(stabils),
    )


def solution(mesh):
    finer = Mesh(mesh.devices.reshape(4, 2, 4, 4, 2), ("zh", "zl", "y", "x", "c"))
    placed = (
        P(TP, None, DP),
        P(DP),
        P(None, DP),
        P(None, DP, TP),
        P(None, DP, TP),
        P(None, DP, TP),
        P(None, DP, TP),
        P(),
        P(),
        P(None, TP),
        P(None, TP, DP),
        P(None, DP, TP, None, None),
        P(None, DP, TP, None),
        P(None, DP, TP),
    )
    return jax.shard_map(
        per_device,
        mesh=finer,
        in_specs=placed,
        out_specs=(
            P(TP, None, DP),
            P(None, DP, TP, None, None),
            P(None, DP, TP, None),
            P(None, DP, TP),
        ),
        check_vma=False,
    )
```

```python
import jax
import jax.numpy as jnp
from jax import lax
from jax.experimental import pallas as pl
from jax.experimental.pallas import tpu as pltpu
from jax.sharding import Mesh
from jax.sharding import PartitionSpec as P

TP = ("zh", "zl", "y")
DP = ("x", "c")
ZZ = ("zl", "zh")
YX = ("y", "x")

EPSILON = 1e-06
NEG_FILL = -1e30
F32 = jnp.float32
BF16 = jnp.bfloat16
EXTRA = 8


def split_pair(value):
    high = value.astype(BF16)
    return high, (value - high.astype(F32)).astype(BF16)


def dot(a, b):
    return lax.dot_general(a, b, (((1,), (0,)), ((), ())), preferred_element_type=F32)


def dot_nt(a, b):
    return lax.dot_general(a, b, (((1,), (1,)), ((), ())), preferred_element_type=F32)


def project_kernel(where, tokens, swapped, gain, gates, *rest):
    weights, out = rest[:-1], rest[-1]
    y, c = where[0], where[1]
    ny = len(weights) // 2
    nx, toks, feat = tokens.shape[1:]
    halves = []
    squares = []
    for source, half in ((tokens, c), (swapped, 1 - c)):
        wide = source[c].reshape(nx * toks, feat).astype(F32)
        halves.append((wide * gain[pl.ds(half, 1), :]).astype(BF16))
        squares.append(split_pair(wide * wide))
    gate_half = [gates[c], gates[1 - c]]
    ones = jnp.ones((8, feat), BF16)
    extras = []
    for xi in range(nx):
        rows = slice(xi * toks, (xi + 1) * toks)
        both = dot_nt(gate_half[0], halves[0][rows]) + dot_nt(gate_half[1], halves[1][rows])
        square = sum(dot_nt(ones, part[rows]) for pair in squares for part in pair)
        extras.append((both, square))
    for k in range(ny):
        head = lax.rem(y + ny - k, ny)
        done = dot(halves[0], weights[2 * k][:feat]) + dot(halves[1], weights[2 * k + 1][:feat])
        out[head, :, :toks, :] = done.astype(BF16).reshape(nx, toks, done.shape[1])
    out[:, :, toks:, :] = jnp.zeros((ny, nx, EXTRA, out.shape[3]), BF16)
    for xi in range(nx):
        both, square = extras[xi]
        high, low = (p.astype(F32) for p in split_pair(both))
        s_high, s_low = (p.astype(F32) for p in split_pair(square))
        for head in range(ny):
            a, b = 2 * head, 2 * head + 1
            block = jnp.concatenate(
                [
                    high[a : a + 1],
                    low[a : a + 1],
                    high[b : b + 1],
                    low[b : b + 1],
                    s_high[0:1],
                    s_low[0:1],
                    jnp.zeros((2, toks), F32),
                ],
                axis=0,
            )
            out[head, xi, toks:, :toks] = block.astype(BF16)


def cell_kernel(width, span, parts, aux, cell, normer, cell_out, normer_out, stabil_out, gated):
    toks = gated.shape[2]
    size = cell.shape[1]
    seqs = toks // span
    total = parts[0, 0].astype(F32)
    for xi in range(1, parts.shape[1]):
        total = total + parts[0, xi].astype(F32)
    rows = jnp.concatenate([total[toks:, :128], aux[0]], axis=0)
    cols = jnp.transpose(rows)[:toks]
    rows = rows[:, :toks]

    def small(get):
        scale = lax.rsqrt((get(4) + get(5)) / width + EPSILON)
        live = get(9) > 0.5
        gate_in = jnp.where(live, scale * (get(0) + get(1)), NEG_FILL)
        forget = scale * (get(2) + get(3)) + get(10)
        log_forget = jnp.minimum(forget, 0.0) - jnp.log1p(jnp.exp(-jnp.abs(forget)))
        return scale, live, gate_in, jnp.where(live, log_forget, 0.0), get(8)

    _, _, in_row, lf_row, m_row = small(lambda i: rows[i : i + 1])
    scale, live, in_col, lf_col, m_col = small(lambda i: cols[:, i : i + 1])
    at_row = lax.broadcasted_iota(jnp.int32, (toks, toks), 0)
    at_col = lax.broadcasted_iota(jnp.int32, (toks, toks), 1)
    same = (at_row // span) == (at_col // span)
    causal = same & (at_col <= at_row)
    anti = same & (at_row <= at_col)
    c_col = jnp.sum(jnp.where(causal, lf_row, 0.0), axis=1, keepdims=True)
    c_row = jnp.sum(jnp.where(anti, lf_col, 0.0), axis=0, keepdims=True)
    last_col = jnp.sum(jnp.where(same, lf_row, 0.0), axis=1, keepdims=True)
    last_row = jnp.sum(jnp.where(same, lf_col, 0.0), axis=0, keepdims=True)
    weight = jnp.where(causal, c_col - c_row + in_row, NEG_FILL)
    carried = c_col + m_col
    running = jnp.maximum(jnp.max(weight, axis=1, keepdims=True), carried)
    carry = jnp.exp(carried - running)

    def piece(i):
        return (scale * total[:toks, i * size : (i + 1) * size]).astype(BF16)

    query, key_vec, value, outgate = (piece(i) for i in range(4))
    shrink = size**-0.5
    scores = dot_nt(query, key_vec) * shrink * jnp.exp(weight - running)
    s_high, s_low = split_pair(scores)
    carried_out = []
    carried_norm = []
    query_wide = query.astype(F32)
    for r in range(seqs):
        at = slice(r * span, (r + 1) * span)
        high, low = split_pair(cell[r])
        carried_out.append(dot(query[at], high) + dot(query[at], low))
        carried_norm.append(jnp.sum(query_wide[at] * normer[0, r : r + 1], axis=1, keepdims=True))
    numer = dot(s_high, value) + dot(s_low, value) + carry * jnp.concatenate(carried_out, axis=0)
    denom = jnp.sum(scores, axis=1, keepdims=True) + carry * jnp.concatenate(carried_norm, axis=0)
    readout = jnp.where(live, numer / jnp.maximum(jnp.abs(denom), 1.0), 0.0)
    mixed = (readout * jax.nn.sigmoid(outgate.astype(F32))).astype(BF16)
    for xi in range(gated.shape[1]):
        gated[0, xi] = mixed

    top_col = jnp.maximum(
        jnp.max(jnp.where(same, last_col - c_row + in_row, NEG_FILL), axis=1, keepdims=True),
        last_col + m_col,
    )
    top_row = jnp.maximum(
        jnp.max(jnp.where(same, last_row - c_col + in_col, NEG_FILL), axis=0, keepdims=True),
        last_row + m_row,
    )
    source = jnp.exp(last_col - c_col + in_col - top_col)
    decay = jnp.exp(last_col + m_col - top_col)
    keyed = (key_vec.astype(F32) * shrink) * source
    k_high, k_low = split_pair(jnp.transpose(keyed))
    token_seq = lax.broadcasted_iota(jnp.int32, (toks, size), 0) // span
    for r in range(seqs):
        at = slice(r * span, (r + 1) * span)
        one = jnp.where(token_seq == r, value.astype(F32), 0.0).astype(BF16)
        fade = decay[r * span : r * span + 1]
        cell_out[r] = fade * cell[r] + (dot(k_high, one) + dot(k_low, one))
        normer_out[0, r : r + 1] = fade * normer[0, r : r + 1] + jnp.sum(
            keyed[at], axis=0, keepdims=True
        )
    stabil_out[0] = jnp.broadcast_to(top_row, (8, toks))


def mix_kernel(where, gated, *rest):
    weights, out = rest[:-1], rest[-1]
    y = where[0]
    ny = len(weights)
    cores, _, nx, toks, size = gated.shape
    for core in range(cores):
        total = None
        for k in range(ny):
            head = lax.rem(y + ny - k, ny)
            part = dot(gated[core, head].reshape(nx * toks, size), weights[k][-size:])
            total = part if total is None else total + part
        out[core] = total.astype(BF16).reshape(nx, toks, total.shape[1])


def add_kernel(parts, own, out, spread):
    total = parts[0].astype(F32)
    for i in range(1, parts.shape[0]):
        total = total + parts[i].astype(F32)
    done = (own[...].astype(F32) + total).astype(BF16)
    out[...] = done
    for i in range(spread.shape[0]):
        spread[i] = done


def pack_kernel(query, key_vec, value, outgate, last, joined, *spread):
    size = query.shape[2]
    feat = query.shape[1]
    for i, source in enumerate((query, key_vec, value, outgate)):
        joined[:feat, i * size : (i + 1) * size] = source[0]
    for copies in spread:
        for i in range(copies.shape[0]):
            copies[i] = last[...]
    if not spread:
        joined[feat:] = last[0]


SMEM_SPEC = pl.BlockSpec(memory_space=pltpu.SMEM)
VMEM_SPEC = pl.BlockSpec(memory_space=pltpu.VMEM)
HBM_SPEC = pl.BlockSpec(memory_space=pltpu.HBM)


def per_device(
    tokens,
    lengths,
    norm_gain,
    query_weight,
    key_weight,
    value_weight,
    outgate_weight,
    input_gate_weight,
    forget_gate_weight,
    forget_bias,
    out_weight,
    cell_state,
    norm_state,
    max_state,
):
    seq_here, span, feat = tokens.shape
    layers, local_seqs, _, size, _ = cell_state.shape
    ny, nx, nc, nz = (lax.axis_size(a) for a in ("y", "x", "c", ZZ))
    toks = seq_here * span
    width = feat * nx * nc
    y, x, c = (lax.axis_index(a) for a in ("y", "x", "c"))
    z = lax.axis_index("zh") * lax.axis_size("zl") + lax.axis_index("zl")
    where = jnp.stack([y, c]).astype(jnp.int32)
    quarters = local_seqs // seq_here

    def shifted(array, step):
        return lax.ppermute(array, "y", [(i, (i + step) % ny) for i in range(ny)])

    def swapped(array):
        return lax.ppermute(array, "c", [(i, (i + 1) % nc) for i in range(nc)])

    gains = lax.all_gather(norm_gain, "c", axis=0)
    live = jnp.arange(span, dtype=jnp.int32)[None, :] < lengths[:, None]

    def aux_of(layer):
        m = jnp.broadcast_to(max_state[layer], (local_seqs, span)).reshape(quarters, 1, toks)
        alive = live.astype(F32).reshape(quarters, 1, toks)
        bias = jnp.broadcast_to(forget_bias[layer, 0], (quarters, 1, toks))
        rows = jnp.concatenate([m, alive, bias, jnp.zeros((quarters, 5, toks), F32)], axis=1)
        return jnp.pad(rows, ((0, 0), (0, 0), (0, 128 - toks)))

    def gates_of(layer):
        cut = [
            lax.dynamic_slice(w[layer], (x * nc * feat, z * ny), (nc * feat, ny))
            for w in (input_gate_weight, forget_gate_weight)
        ]
        both = jnp.stack(cut, axis=2).reshape(nc, feat, 2 * ny)
        return jnp.transpose(both, (0, 2, 1))

    projections = (query_weight, key_weight, value_weight, outgate_weight)
    current = tokens.reshape(toks, feat)

    def pack(layer, last, last_spec, out_shape):
        whole = [pl.BlockSpec(o.shape, lambda i, n=len(o.shape): (0,) * n) for o in out_shape]
        return pl.pallas_call(
            pack_kernel,
            grid=(1,),
            out_shape=out_shape,
            in_specs=[pl.BlockSpec((1, feat, size), lambda i: (layer, 0, 0))] * 4 + [last_spec],
            out_specs=whole,
            compiler_params=pltpu.CompilerParams(vmem_limit_bytes=60 << 20),
        )(*projections, last)

    joined, spread = pack(
        0,
        current,
        pl.BlockSpec((toks, feat), lambda i: (0, 0)),
        [
            jax.ShapeDtypeStruct((feat, 4 * size), BF16),
            jax.ShapeDtypeStruct((nz, toks, feat), BF16),
        ],
    )
    spread = spread.reshape(nz * toks, feat)
    moved = [joined] + [shifted(joined, k) for k in range(1, ny)]
    own_out, moved[ny // 2] = lax.optimization_barrier((out_weight[0], moved[ny // 2]))
    outs = [own_out] + [shifted(own_out, k) for k in range(1, ny)]
    weights = []
    for w in moved:
        weights += [w, swapped(w)]
    states = []
    for layer in range(layers):
        arrived = lax.all_to_all(spread, ZZ, 0, 0, tiled=True)
        if layer == 0:
            (packed,) = pack(
                1,
                out_weight,
                pl.BlockSpec((1, size, feat), lambda i: (1, 0, 0)),
                [jax.ShapeDtypeStruct((feat + size, 4 * size), BF16)],
            )
            auxes = [aux_of(n) for n in range(layers)]
            gates = [gates_of(n) for n in range(layers)]
            gains = [gains[:, n] for n in range(layers)]
            (arrived, auxes, gates, gains, where, packed) = lax.optimization_barrier(
                (arrived, auxes, gates, gains, where, packed)
            )
        other = swapped(arrived).reshape(nc, nx, toks, feat)
        arrived = arrived.reshape(nc, nx, toks, feat)
        parts = pl.pallas_call(
            project_kernel,
            out_shape=jax.ShapeDtypeStruct((ny, nx, toks + EXTRA, 4 * size), BF16),
            in_specs=[SMEM_SPEC] + [VMEM_SPEC] * (4 + 2 * ny),
            out_specs=VMEM_SPEC,
            compiler_params=pltpu.CompilerParams(vmem_limit_bytes=16 << 20),
        )(where, arrived, other, gains[layer], gates[layer], *weights)
        summed = lax.all_to_all(
            parts.reshape(ny * nx * (toks + EXTRA), 4 * size), YX, 0, 0, tiled=True
        ).reshape(ny, nx, toks + EXTRA, 4 * size)
        first = layer * quarters
        state_specs = (
            pl.BlockSpec((seq_here, size, size), lambda i: (first + i, 0, 0)),
            pl.BlockSpec((1, seq_here, size), lambda i: (first + i, 0, 0)),
            pl.BlockSpec((1, 8, toks), lambda i: (first + i, 0, 0)),
        )
        kept = [HBM_SPEC] * len(states)
        *states, gated = pl.pallas_call(
            lambda *refs: cell_kernel(width, span, *refs[:4], *refs[4 + len(kept) :]),
            grid=(quarters,),
            out_shape=(
                jax.ShapeDtypeStruct((layers * local_seqs, size, size), F32),
                jax.ShapeDtypeStruct((layers * quarters, seq_here, size), F32),
                jax.ShapeDtypeStruct((layers * quarters, 8, toks), F32),
                jax.ShapeDtypeStruct((quarters, nx, toks, size), BF16),
            ),
            in_specs=[
                pl.BlockSpec((1, nx, toks + EXTRA, 4 * size), lambda i: (i, 0, 0, 0)),
                pl.BlockSpec((1, 8, 128), lambda i: (i, 0, 0)),
                *state_specs[:2],
                *kept,
            ],
            out_specs=(
                *state_specs,
                pl.BlockSpec((1, nx, toks, size), lambda i: (i, 0, 0, 0)),
            ),
            input_output_aliases={4 + n: n for n in range(len(kept))},
            compiler_params=pltpu.CompilerParams(vmem_limit_bytes=10 << 20),
        )(
            summed,
            auxes[layer],
            cell_state.reshape(layers * local_seqs, size, size),
            norm_state.reshape(layers * quarters, seq_here, size),
            *states,
        )
        if layer + 1 < layers:
            packed, gated = lax.optimization_barrier((packed, gated))
        heads = lax.all_to_all(
            gated.reshape(quarters * nx * toks, size), YX, 0, 0, tiled=True
        ).reshape(ny, nx, toks, size)
        if layer + 1 < layers:
            moved = [packed] + [shifted(packed, k) for k in range(1, ny)]
            weights = []
            for w in moved:
                weights += [w, swapped(w)]
            next_outs = moved
        everyone = lax.all_gather(heads, "c", axis=0)
        mixed = pl.pallas_call(
            mix_kernel,
            out_shape=jax.ShapeDtypeStruct((nc, nx, toks, feat), BF16),
            in_specs=[SMEM_SPEC] + [VMEM_SPEC] * (1 + ny),
            out_specs=VMEM_SPEC,
            compiler_params=pltpu.CompilerParams(vmem_limit_bytes=8 << 20),
        )(where, everyone, *outs)
        mixed = mixed.reshape(nz * toks, feat)
        added = lax.all_to_all(mixed, ZZ, 0, 0, tiled=True).reshape(nz, toks, feat)
        outs = next_outs
        current, spread = pl.pallas_call(
            add_kernel,
            out_shape=(
                jax.ShapeDtypeStruct((toks, feat), BF16),
                jax.ShapeDtypeStruct((nz, toks, feat), BF16),
            ),
            in_specs=[VMEM_SPEC] * 2,
            out_specs=(VMEM_SPEC, VMEM_SPEC),
            compiler_params=pltpu.CompilerParams(vmem_limit_bytes=8 << 20),
        )(added, current)
        spread = spread.reshape(nz * toks, feat)
    cell_next, normer_next, top = states
    return (
        current.reshape(seq_here, span, feat),
        cell_next.reshape(cell_state.shape),
        normer_next.reshape(norm_state.shape),
        top[:, 0, ::span].reshape(max_state.shape),
    )


def solution(mesh):
    finer = Mesh(mesh.devices.reshape(4, 2, 4, 4, 2), ("zh", "zl", "y", "x", "c"))
    placed = (
        P(TP, None, DP),
        P(DP),
        P(None, DP),
        P(None, DP, TP),
        P(None, DP, TP),
        P(None, DP, TP),
        P(None, DP, TP),
        P(),
        P(),
        P(None, TP),
        P(None, TP, DP),
        P(None, DP, TP, None, None),
        P(None, DP, TP, None),
        P(None, DP, TP),
    )

    return jax.shard_map(
        per_device,
        mesh=finer,
        in_specs=placed,
        out_specs=(
            P(TP, None, DP),
            P(None, DP, TP, None, None),
            P(None, DP, TP, None),
            P(None, DP, TP),
        ),
        check_vma=False,
    )
```

```python
import jax
import jax.numpy as jnp
from jax import lax
from jax.experimental import pallas as pl
from jax.experimental.pallas import tpu as pltpu
from jax.sharding import Mesh
from jax.sharding import PartitionSpec as P

TP = ("zh", "zl", "y")
DP = ("x", "c")
ZZ = ("zl", "zh")
YX = ("y", "x")

EPSILON = 1e-06
NEG_FILL = -1e30
F32 = jnp.float32
BF16 = jnp.bfloat16
EXTRA = 8
LIVE = 896


def split_pair(value):
    high = value.astype(BF16)
    return high, (value - high.astype(F32)).astype(BF16)


def dot(a, b):
    return lax.dot_general(a, b, (((1,), (0,)), ((), ())), preferred_element_type=F32)


def dot_nt(a, b):
    return lax.dot_general(a, b, (((1,), (1,)), ((), ())), preferred_element_type=F32)


def dot_tn(a, b):
    return lax.dot_general(a, b, (((0,), (0,)), ((), ())), preferred_element_type=F32)


def places(kk, base, ways, toks):
    per = toks // ways
    row = lax.broadcasted_iota(jnp.int32, (toks, toks), 0)
    turn = row // per + ways - base.astype(jnp.int32)
    turn = jnp.where(turn >= ways, turn - ways, turn)
    return (ways * (row % per) + turn == kk.astype(jnp.int32)).astype(BF16)


def chosen(rank, count):
    at = lax.broadcasted_iota(jnp.int32, (count, rank.shape[1]), 0)
    return (at == rank.astype(jnp.int32)).astype(BF16)


def project_kernel(layer, nx, toks, where, *refs):
    tokens, swapped, rank, gain, gain_other, gate_in, gate_forget, *weights, out, held, near, sems = refs
    y, c, z = where[0], where[1], where[3]
    ny = len(weights) // 2
    heads = gate_in.shape[1]
    feat = tokens.shape[-1]
    copies = [
        pltpu.make_async_copy(w.at[:feat], near.at[n], sems.at[n]) for n, w in enumerate(weights)
    ]
    for copy in copies:
        copy.start()
    halves = []
    squares = []
    compact = len(tokens.shape) == 2
    if compact:
        pick = chosen(rank[pl.ds(c, 1), :], tokens.shape[0])
    for source, scales in ((tokens, gain), (swapped, gain_other)):
        if compact:
            wide = dot_tn(pick, source[...])
        else:
            wide = source[c].reshape(nx * toks, feat).astype(F32)
        halves.append((wide * scales[layer : layer + 1]).astype(BF16))
        squares.append(split_pair(wide * wide))
    gates = jnp.concatenate([gate_in[0], gate_forget[0]], axis=0)
    low, high = gates[:, :feat], gates[:, feat:]
    gate_half = [jnp.where(c == 0, low, high), jnp.where(c == 0, high, low)]
    ones = jnp.ones((8, feat), BF16)
    extras = []
    for xi in range(nx):
        rows = slice(xi * toks, (xi + 1) * toks)
        both = dot_nt(gate_half[0], halves[0][rows]) + dot_nt(gate_half[1], halves[1][rows])
        square = sum(dot_nt(ones, part[rows]) for pair in squares for part in pair)
        held[xi] = both
        extras.append(square)
    for k in range(ny):
        head = lax.rem(y + ny - k, ny)
        copies[2 * k].wait()
        copies[2 * k + 1].wait()
        done = dot(halves[0], near[2 * k]) + dot(halves[1], near[2 * k + 1])
        out[head, :, :toks, :] = done.astype(BF16).reshape(nx, toks, done.shape[1])
    out[:, :, toks:, :] = jnp.zeros((ny, nx, EXTRA, out.shape[3]), BF16)
    for xi in range(nx):
        s_high, s_low = (p.astype(F32) for p in split_pair(extras[xi]))
        for head in range(ny):
            values = []
            for kind in range(2):
                row = held[xi, pl.ds(kind * heads + z * ny + head, 1), :]
                values += [p.astype(F32) for p in split_pair(row)]
            block = jnp.concatenate(
                [
                    *values,
                    s_high[0:1],
                    s_low[0:1],
                    jnp.zeros((2, toks), F32),
                ],
                axis=0,
            )
            out[head, xi, toks:, :toks] = block.astype(BF16)


def cell_kernel(width, span, classed, parts, extras, aux, cell, normer, cell_out, normer_out, stabil_out, gated):
    ways = parts.shape[0] if classed else gated.shape[0]
    toks = gated.shape[2] if classed else gated.shape[2] * ways
    size = cell.shape[1]
    seqs = toks // span
    place = places(aux[0, 3:4, :toks], aux[0, 4:5, :toks], ways, toks)
    if classed:
        per = toks // ways
        wide = parts[:, 0].astype(F32)
        more = extras[:, 0, :, :128].astype(F32)
        for xi in range(1, parts.shape[1]):
            wide = wide + parts[:, xi].astype(F32)
            more = more + extras[:, xi, :, :128].astype(F32)
        high, low = split_pair(wide.reshape(toks, wide.shape[2]))
        total = dot_tn(place, high) + dot_tn(place, low)
        kk = aux[0, 3:4, :toks].astype(jnp.int32)
        at = kk + aux[0, 4:5, :toks].astype(jnp.int32)
        at = at - at // ways * ways
        at = at * 128 + pl.program_id(0) * per + kk // ways
        at = jnp.where(kk < 0, -1, at)
        lane = lax.broadcasted_iota(jnp.int32, (ways * 128, toks), 0)
        move = (lane == at).astype(BF16)
        more = jnp.concatenate([more[way] for way in range(ways)], axis=1)
        extra = jnp.zeros((EXTRA, toks), F32)
        for _ in range(3):
            now = more.astype(BF16)
            extra = extra + dot(now, move)
            more = more - now.astype(F32)
        extra = jnp.concatenate([extra, jnp.zeros((EXTRA, 128 - toks), F32)], axis=1)
    else:
        total = parts[0, 0].astype(F32)
        for xi in range(1, parts.shape[1]):
            total = total + parts[0, xi].astype(F32)
        extra = total[toks:, :128]
    rows = jnp.concatenate([extra, aux[0]], axis=0)
    cols = jnp.transpose(rows)[:toks]
    rows = rows[:, :toks]

    def small(get):
        scale = lax.rsqrt((get(4) + get(5)) / width + EPSILON)
        live = get(9) > 0.5
        gate_in = jnp.where(live, scale * (get(0) + get(1)), NEG_FILL)
        forget = scale * (get(2) + get(3)) + get(10)
        log_forget = jnp.minimum(forget, 0.0) - jnp.log1p(jnp.exp(-jnp.abs(forget)))
        return scale, live, gate_in, jnp.where(live, log_forget, 0.0), get(8)

    _, _, in_row, lf_row, m_row = small(lambda i: rows[i : i + 1])
    scale, live, in_col, lf_col, m_col = small(lambda i: cols[:, i : i + 1])
    at_row = lax.broadcasted_iota(jnp.int32, (toks, toks), 0)
    at_col = lax.broadcasted_iota(jnp.int32, (toks, toks), 1)
    same = (at_row // span) == (at_col // span)
    causal = same & (at_col <= at_row)
    anti = same & (at_row <= at_col)
    c_col = jnp.sum(jnp.where(causal, lf_row, 0.0), axis=1, keepdims=True)
    c_row = jnp.sum(jnp.where(anti, lf_col, 0.0), axis=0, keepdims=True)
    last_col = jnp.sum(jnp.where(same, lf_row, 0.0), axis=1, keepdims=True)
    last_row = jnp.sum(jnp.where(same, lf_col, 0.0), axis=0, keepdims=True)
    weight = jnp.where(causal, c_col - c_row + in_row, NEG_FILL)
    carried = c_col + m_col
    running = jnp.maximum(jnp.max(weight, axis=1, keepdims=True), carried)
    carry = jnp.exp(carried - running)

    def piece(i):
        return (scale * total[:toks, i * size : (i + 1) * size]).astype(BF16)

    query, key_vec, value, outgate = (piece(i) for i in range(4))
    shrink = size**-0.5
    scores = dot_nt(query, key_vec) * shrink * jnp.exp(weight - running)
    s_high, s_low = split_pair(scores)
    carried_out = []
    carried_norm = []
    query_wide = query.astype(F32)
    for r in range(seqs):
        at = slice(r * span, (r + 1) * span)
        high, low = split_pair(cell[r])
        carried_out.append(dot(query[at], high) + dot(query[at], low))
        carried_norm.append(jnp.sum(query_wide[at] * normer[0, r : r + 1], axis=1, keepdims=True))
    numer = dot(s_high, value) + dot(s_low, value) + carry * jnp.concatenate(carried_out, axis=0)
    denom = jnp.sum(scores, axis=1, keepdims=True) + carry * jnp.concatenate(carried_norm, axis=0)
    readout = jnp.where(live, numer / jnp.maximum(jnp.abs(denom), 1.0), 0.0)
    mixed = (readout * jax.nn.sigmoid(outgate.astype(F32))).astype(BF16)
    if not classed:
        mixed = dot(place, mixed).astype(BF16).reshape(ways, toks // ways, size)
    for xi in range(gated.shape[1]):
        if classed:
            gated[0, xi] = mixed
        else:
            gated[:, xi] = mixed

    top_col = jnp.maximum(
        jnp.max(jnp.where(same, last_col - c_row + in_row, NEG_FILL), axis=1, keepdims=True),
        last_col + m_col,
    )
    top_row = jnp.maximum(
        jnp.max(jnp.where(same, last_row - c_col + in_col, NEG_FILL), axis=0, keepdims=True),
        last_row + m_row,
    )
    source = jnp.exp(last_col - c_col + in_col - top_col)
    decay = jnp.exp(last_col + m_col - top_col)
    keyed = (key_vec.astype(F32) * shrink) * source
    k_high, k_low = split_pair(jnp.transpose(keyed))
    token_seq = lax.broadcasted_iota(jnp.int32, (toks, size), 0) // span
    for r in range(seqs):
        at = slice(r * span, (r + 1) * span)
        one = jnp.where(token_seq == r, value.astype(F32), 0.0).astype(BF16)
        fade = decay[r * span : r * span + 1]
        cell_out[r] = fade * cell[r] + (dot(k_high, one) + dot(k_low, one))
        normer_out[0, r : r + 1] = fade * normer[0, r : r + 1] + jnp.sum(
            keyed[at], axis=0, keepdims=True
        )
    stabil_out[0] = jnp.broadcast_to(top_row, (8, toks))


def gather_kernel(where, gated, rank, rank_here, own, *rest):
    weights, out = rest[:-1], rest[-1]
    y = where[0]
    ny = len(weights)
    cores, _, nx, toks, size = gated.shape
    total = dot(chosen(rank_here[0:1, :], out.shape[0]), own[...])
    picks = [chosen(rank[i : i + 1, :], out.shape[0]) for i in range(cores)]
    for k in range(ny):
        head = lax.rem(y + ny - k, ny)
        rows = sum(
            dot(picks[i], gated[i, head].reshape(nx * toks, size)) for i in range(cores)
        ).astype(BF16)
        total = total + dot(rows, weights[k][-size:])
    out[...] = total.astype(BF16)


def mix_kernel(where, gated, *rest):
    weights, out = rest[:-1], rest[-1]
    y = where[0]
    ny = len(weights)
    cores, _, nx, toks, size = gated.shape
    for core in range(cores):
        total = None
        for k in range(ny):
            head = lax.rem(y + ny - k, ny)
            part = dot(gated[core, head].reshape(nx * toks, size), weights[k][-size:])
            total = part if total is None else total + part
        out[core] = total.astype(BF16).reshape(nx, toks, total.shape[1])


def add_kernel(parts, spread):
    total = parts[0].astype(F32)
    for i in range(1, parts.shape[0]):
        total = total + parts[i].astype(F32)
    done = total.astype(BF16)
    for i in range(spread.shape[0]):
        spread[i] = done


def last_kernel(ways, parts, rows, tokens, home, out):
    total = parts[0].astype(F32)
    for i in range(1, parts.shape[0]):
        total = total + parts[i].astype(F32)
    toks = tokens.shape[0]
    place = places(home[0:1, :toks], home[1:2, :toks], ways, toks)
    own = dot_tn(place, rows[...])
    alive = dot_tn(place, jnp.ones(rows.shape, BF16))
    out[...] = jnp.where(alive > 0.5, own + total, tokens[...].astype(F32)).astype(BF16)


def index_kernel(groups, span, where, bias, tops, own, *rest):
    came, (aux, rank, rank_here, home) = rest[:-4], rest[-4:]
    y, x, z = where[0], where[2], where[3]
    nx = len(came)
    quarters, seqs = own.shape
    toks = seqs * span
    lanes = groups * quarters

    def grid(rows, cols):
        return (
            lax.broadcasted_iota(jnp.int32, (rows, cols), 0),
            lax.broadcasted_iota(jnp.int32, (rows, cols), 1),
        )

    def times(mask, value):
        return dot(mask.astype(BF16), value.astype(BF16))

    def spread_seqs(some):
        at = grid(some.shape[0], toks)[1] // span
        return sum(jnp.where(at == r, some[:, r : r + 1], 0.0) for r in range(seqs))

    def numbered(some):
        _, lane = grid(some.shape[0], toks)
        before = sum(
            jnp.where(lane // span > r, some[:, r : r + 1], 0.0) for r in range(seqs - 1)
        )
        slot = lane % span
        live = slot.astype(F32) < spread_seqs(some)
        return jnp.where(live, before + slot.astype(F32), -1.0), live

    def turned(value):
        return value - quarters * jnp.floor(value * (1.0 / quarters))

    def base_of(some):
        row, col = grid(some.shape[0], some.shape[0])
        held = jnp.sum(some, axis=1, keepdims=True)
        earlier = (row // quarters == col // quarters) & (col < row)
        base = times(earlier, jnp.broadcast_to(held, (some.shape[0], 128)))[:, :1]
        return turned(base), held

    mine = own[...].astype(F32)
    kk, live = numbered(mine)
    base, _ = base_of(mine)
    aux[...] = jnp.zeros(aux.shape, F32)
    for layer in range(aux.shape[0]):
        top = spread_seqs(tops[layer])
        for q in range(quarters):
            aux[layer, q, 0:1, :toks] = top[q : q + 1]
            aux[layer, q, 1:2, :toks] = live[q : q + 1].astype(F32)
            aux[layer, q, 2:3, :toks] = jnp.full((1, toks), bias[layer], F32)
            aux[layer, q, 3:4, :toks] = kk[q : q + 1]
            aux[layer, q, 4:5, :toks] = jnp.broadcast_to(base[q : q + 1], (1, toks))

    row, col = grid(lanes, came[0].shape[0])
    everyone = jnp.zeros((lanes, seqs), F32)
    for k in range(nx):
        from_x = lax.rem(x + nx - k, nx)
        cores = groups // nx
        hit = (row // (quarters * cores) == from_x) & (row % (quarters * cores) == col)
        everyone = everyone + times(hit, came[k][...])
    kk_all, _ = numbered(everyone)
    base_all, held_all = base_of(everyone)
    here = grid(lanes, toks)[0] == z * quarters + y
    home[...] = jnp.zeros(home.shape, F32)
    home[0:1] = jnp.sum(jnp.where(here, kk_all, 0.0), axis=0, keepdims=True)
    home[1:2] = jnp.sum(jnp.where(here, base_all, 0.0), axis=0, keepdims=True)

    per = toks // quarters
    turn = turned(y.astype(F32) + quarters - base_all)
    lane = grid(lanes, 128)[1]
    alive = (quarters * lane.astype(F32) + turn < held_all) & (lane < per)
    up, down = grid(128, 128)
    inside = times(alive, (up < down).astype(F32))
    held = jnp.broadcast_to(
        jnp.sum(alive.astype(F32), axis=1, keepdims=True), (lanes, 128)
    )
    up, down = grid(lanes, lanes)
    order = jnp.where(alive, inside + times(down < up, held), -1.0)
    ranks = jnp.zeros((groups, toks), F32)
    for q in range(quarters):
        up, down = grid(groups, lanes)
        picked = times(down == up * quarters + q, order)
        up, down = grid(128, toks)
        ranks = ranks + dot(picked.astype(BF16), (down == up + q * per).astype(BF16)) * (
            grid(groups, toks)[1] // per == q
        ).astype(F32)
    at = grid(groups, toks)[0] == z
    rank_here[...] = jnp.broadcast_to(
        jnp.sum(jnp.where(at, ranks, 0.0), axis=0, keepdims=True), rank_here.shape
    )
    cores, wide = rank.shape
    for core in range(cores):
        total = jnp.zeros((8, wide), F32)
        for xi in range(nx):
            one = jnp.broadcast_to(ranks[cores * xi + core : cores * xi + core + 1], (8, toks))
            up, down = grid(toks, wide)
            total = total + dot(one.astype(BF16), (down == up + xi * toks).astype(BF16))
        rank[core : core + 1] = total[:1]


def pack_kernel(query, key_vec, value, outgate, last, joined, *spread):
    size = query.shape[2]
    feat = query.shape[1]
    for i, source in enumerate((query, key_vec, value, outgate)):
        joined[:feat, i * size : (i + 1) * size] = source[0]
    for copies in spread:
        for i in range(copies.shape[0]):
            copies[i] = last[...]
    if not spread:
        joined[feat:] = last[0]


SMEM_SPEC = pl.BlockSpec(memory_space=pltpu.SMEM)
VMEM_SPEC = pl.BlockSpec(memory_space=pltpu.VMEM)
HBM_SPEC = pl.BlockSpec(memory_space=pltpu.HBM)


def per_device(
    tokens,
    lengths,
    norm_gain,
    query_weight,
    key_weight,
    value_weight,
    outgate_weight,
    input_gate_weight,
    forget_gate_weight,
    forget_bias,
    out_weight,
    cell_state,
    norm_state,
    max_state,
):
    seq_here, span, feat = tokens.shape
    layers, local_seqs, _, size, _ = cell_state.shape
    heads_all = input_gate_weight.shape[2]
    ny, nx, nc, nz = (lax.axis_size(a) for a in ("y", "x", "c", ZZ))
    toks = seq_here * span
    width = feat * nx * nc
    y, x, c = (lax.axis_index(a) for a in ("y", "x", "c"))
    z = lax.axis_index("zh") * lax.axis_size("zl") + lax.axis_index("zl")
    where = jnp.stack([y, c, x, z]).astype(jnp.int32)
    quarters = local_seqs // seq_here

    def shifted(array, step):
        return lax.ppermute(array, "y", [(i, (i + step) % ny) for i in range(ny)])

    def swapped(array):
        return lax.ppermute(array, "c", [(i, (i + 1) % nc) for i in range(nc)])

    def exchanged(rows):
        height = toks // ny
        came = [
            shifted(lax.dynamic_slice(rows, ((y + k) % ny * height, 0), (height, feat)), k)
            if k
            else lax.dynamic_slice(rows, (y * height, 0), (height, feat))
            for k in range(ny)
        ]
        came = jnp.concatenate(came, axis=0)
        return jnp.concatenate(
            [
                lax.dynamic_slice(came, ((y + ny - q) % ny * height, 0), (height, feat))
                for q in range(ny)
            ],
            axis=0,
        )

    gain_other = swapped(norm_gain)
    gate_weights = [
        jnp.transpose(w, (0, 2, 1)) for w in (input_gate_weight, forget_gate_weight)
    ]
    pair = swapped(lengths)
    pair = jnp.where(c == 0, jnp.stack([lengths, pair]), jnp.stack([pair, lengths]))
    turned = [pair] + [
        lax.ppermute(pair, "x", [(i, (i + k) % nx) for i in range(nx)]) for k in range(1, nx)
    ]
    per = toks // ny
    live = [t.reshape(nc * quarters, seq_here) for t in turned]
    auxes, rank, rank_here, home = pl.pallas_call(
        lambda *refs: index_kernel(nx * nc, span, *refs),
        out_shape=(
            jax.ShapeDtypeStruct((layers, quarters, 8, 128), F32),
            jax.ShapeDtypeStruct((nc, nx * toks), F32),
            jax.ShapeDtypeStruct((8, toks), F32),
            jax.ShapeDtypeStruct((8, toks), F32),
        ),
        in_specs=[SMEM_SPEC] * 2 + [VMEM_SPEC] * (2 + nx),
        out_specs=(VMEM_SPEC,) * 4,
        compiler_params=pltpu.CompilerParams(vmem_limit_bytes=4 << 20),
        name="index",
    )(
        where,
        forget_bias.reshape(layers),
        max_state.reshape(layers, quarters, seq_here),
        lengths.reshape(quarters, seq_here),
        *live,
    )
    compact = -(-(LIVE // ny + nz) // (16 * nz)) * 16 * nz

    projections = (query_weight, key_weight, value_weight, outgate_weight)
    current = tokens.reshape(toks, feat)

    def pack(layer, last, last_spec, out_shape):
        whole = [pl.BlockSpec(o.shape, lambda i, n=len(o.shape): (0,) * n) for o in out_shape]
        return pl.pallas_call(
            pack_kernel,
            grid=(1,),
            out_shape=out_shape,
            in_specs=[pl.BlockSpec((1, feat, size), lambda i: (layer, 0, 0))] * 4 + [last_spec],
            out_specs=whole,
            compiler_params=pltpu.CompilerParams(vmem_limit_bytes=60 << 20),
        )(*projections, last)

    joined, spread = pack(
        0,
        current,
        pl.BlockSpec((toks, feat), lambda i: (0, 0)),
        [
            jax.ShapeDtypeStruct((feat, 4 * size), BF16),
            jax.ShapeDtypeStruct((nz, toks, feat), BF16),
        ],
    )
    spread = spread.reshape(nz * toks, feat)
    moved = [joined] + [shifted(joined, k) for k in range(1, ny)]
    weights = []
    for w in moved:
        weights += [w, swapped(w)]
    states = []
    for layer in range(layers):
        arrived = lax.all_to_all(spread, ZZ, 0, 0, tiled=True)
        if layer == 0:
            (packed,) = pack(
                1,
                out_weight,
                pl.BlockSpec((1, size, feat), lambda i: (1, 0, 0)),
                [jax.ShapeDtypeStruct((feat + size, 4 * size), BF16)],
            )
            arrived, packed = lax.optimization_barrier((arrived, packed))
            rows = dot(places(home[0:1], home[1:2], ny, toks), current).astype(BF16)
        other = swapped(arrived)
        if layer:
            rows = dot_tn(chosen(rank_here[0:1], compact), arrived).astype(BF16)
        if layer == 0:
            other = other.reshape(nc, nx, toks, feat)
            arrived = arrived.reshape(nc, nx, toks, feat)
        whole = [
            pl.BlockSpec(a.shape, lambda i, w, n=a.ndim: (0,) * n)
            for a in (arrived, other, rank, norm_gain, gain_other)
        ]
        gate_spec = pl.BlockSpec((1, heads_all, nc * feat), lambda i, w: (layer, 0, w[2]))
        out_shape = (ny, nx, toks + EXTRA, 4 * size)
        parts = pl.pallas_call(
            lambda *refs: project_kernel(layer, nx, toks, *refs),
            out_shape=jax.ShapeDtypeStruct(out_shape, BF16),
            grid_spec=pltpu.PrefetchScalarGridSpec(
                num_scalar_prefetch=1,
                grid=(1,),
                in_specs=whole + [gate_spec] * 2 + [HBM_SPEC] * (2 * ny),
                out_specs=pl.BlockSpec(out_shape, lambda i, w: (0, 0, 0, 0)),
                scratch_shapes=[
                    pltpu.VMEM((nx, 2 * heads_all, toks), F32),
                    pltpu.VMEM((2 * ny, feat, 4 * size), BF16),
                    pltpu.SemaphoreType.DMA((2 * ny,)),
                ],
            ),
            compiler_params=pltpu.CompilerParams(vmem_limit_bytes=60 << 20),
        )(where, arrived, other, rank, norm_gain, gain_other, *gate_weights, *weights)
        rows = exchanged(rows)
        summed = lax.all_to_all(
            parts.reshape(ny * nx * (toks + EXTRA), 4 * size), YX, 0, 0, tiled=True
        ).reshape(ny, nx, toks + EXTRA, 4 * size)
        if layer == 0:
            rows, summed = lax.optimization_barrier((rows, summed))
        if layer == 0:
            outs = [out_weight[0]] + [shifted(out_weight[0], k) for k in range(1, ny)]
            near = {k: shifted(packed, k) for k in (1, ny - 1)}
        first = layer * quarters
        state_specs = (
            pl.BlockSpec((seq_here, size, size), lambda i: (first + i, 0, 0)),
            pl.BlockSpec((1, seq_here, size), lambda i: (first + i, 0, 0)),
            pl.BlockSpec((1, 8, toks), lambda i: (first + i, 0, 0)),
        )
        kept = [HBM_SPEC] * len(states)
        part_block = (1, nx, toks + EXTRA, 4 * size)
        part_spec = pl.BlockSpec(part_block, lambda i: (i, 0, 0, 0))
        extra_at = (0, 0, 0, 0)
        send_spec = pl.BlockSpec((ny, nx, per, size), lambda i: (0, 0, i, 0))
        if layer:
            part_spec = pl.BlockSpec((ny, nx, per, 4 * size), lambda i: (0, 0, i, 0))
            extra_at = (0, 0, toks // EXTRA, 0)
            send_spec = pl.BlockSpec((1, nx, toks, size), lambda i: (i, 0, 0, 0))
        *states, gated = pl.pallas_call(
            lambda *refs: cell_kernel(
                width, span, layer > 0, *refs[:5], *refs[5 + len(kept) :]
            ),
            grid=(quarters,),
            out_shape=(
                jax.ShapeDtypeStruct((layers * local_seqs, size, size), F32),
                jax.ShapeDtypeStruct((layers * quarters, seq_here, size), F32),
                jax.ShapeDtypeStruct((layers * quarters, 8, toks), F32),
                jax.ShapeDtypeStruct((quarters, nx, toks, size), BF16),
            ),
            in_specs=[
                part_spec,
                pl.BlockSpec((ny, nx, EXTRA, 4 * size), lambda i: extra_at),
                pl.BlockSpec((1, 8, 128), lambda i: (first + i, 0, 0)),
                *state_specs[:2],
                *kept,
            ],
            out_specs=(
                *state_specs,
                send_spec,
            ),
            input_output_aliases={5 + n: n for n in range(len(kept))},
            compiler_params=pltpu.CompilerParams(vmem_limit_bytes=10 << 20),
        )(
            summed,
            summed,
            auxes.reshape(layers * quarters, 8, 128),
            cell_state.reshape(layers * local_seqs, size, size),
            norm_state.reshape(layers * quarters, seq_here, size),
            *states,
        )
        heads = lax.all_to_all(
            gated.reshape(quarters * nx * toks, size), YX, 0, 0, tiled=True
        ).reshape(ny, nx, toks, size)
        if layer + 1 < layers:
            late, heads = lax.optimization_barrier((packed, heads))
            far = {k: shifted(late, k) for k in range(2, ny - 1)}
            moved = [packed] + [(near | far)[k] for k in range(1, ny)]
            weights = []
            for w in moved:
                weights += [w, swapped(w)]
            next_outs = moved
        everyone = lax.all_gather(heads, "c", axis=0)
        if layer + 1 < layers:
            mixed = pl.pallas_call(
                gather_kernel,
                out_shape=jax.ShapeDtypeStruct((compact, feat), BF16),
                in_specs=[SMEM_SPEC] + [VMEM_SPEC] * (4 + ny),
                out_specs=VMEM_SPEC,
                compiler_params=pltpu.CompilerParams(vmem_limit_bytes=60 << 20),
            )(where, everyone, rank, rank_here, rows, *outs)
            added = lax.all_to_all(mixed, ZZ, 0, 0, tiled=True)
            spread = pl.pallas_call(
                add_kernel,
                out_shape=jax.ShapeDtypeStruct((nz, compact // nz, feat), BF16),
                in_specs=[VMEM_SPEC],
                out_specs=VMEM_SPEC,
                compiler_params=pltpu.CompilerParams(vmem_limit_bytes=8 << 20),
            )(added.reshape(nz, compact // nz, feat))
            spread = spread.reshape(compact, feat)
            outs = next_outs
            continue
        mixed = pl.pallas_call(
            mix_kernel,
            out_shape=jax.ShapeDtypeStruct((nc, nx, toks, feat), BF16),
            in_specs=[SMEM_SPEC] + [VMEM_SPEC] * (1 + ny),
            out_specs=VMEM_SPEC,
            compiler_params=pltpu.CompilerParams(vmem_limit_bytes=8 << 20),
        )(where, everyone, *outs)
        added = lax.all_to_all(mixed.reshape(nz * toks, feat), ZZ, 0, 0, tiled=True)
        current = pl.pallas_call(
            lambda *refs: last_kernel(ny, *refs),
            out_shape=jax.ShapeDtypeStruct((toks, feat), BF16),
            in_specs=[VMEM_SPEC] * 4,
            out_specs=VMEM_SPEC,
            compiler_params=pltpu.CompilerParams(vmem_limit_bytes=8 << 20),
        )(added.reshape(nz, toks, feat), rows, current, home)
    cell_next, normer_next, top = states
    return (
        current.reshape(seq_here, span, feat),
        cell_next.reshape(cell_state.shape),
        normer_next.reshape(norm_state.shape),
        top[:, 0, ::span].reshape(max_state.shape),
    )


def solution(mesh):
    finer = Mesh(mesh.devices.reshape(4, 2, 4, 4, 2), ("zh", "zl", "y", "x", "c"))
    placed = (
        P(TP, None, DP),
        P(DP),
        P(None, DP),
        P(None, DP, TP),
        P(None, DP, TP),
        P(None, DP, TP),
        P(None, DP, TP),
        P(),
        P(),
        P(None, TP),
        P(None, TP, DP),
        P(None, DP, TP, None, None),
        P(None, DP, TP, None),
        P(None, DP, TP),
    )

    return jax.shard_map(
        per_device,
        mesh=finer,
        in_specs=placed,
        out_specs=(
            P(TP, None, DP),
            P(None, DP, TP, None, None),
            P(None, DP, TP, None),
            P(None, DP, TP),
        ),
        check_vma=False,
    )
```

```python
import jax
import jax.numpy as jnp
from jax import lax
from jax.experimental import pallas as pl
from jax.experimental.pallas import tpu as pltpu
from jax.sharding import Mesh
from jax.sharding import PartitionSpec as P

TP = ("zh", "zl", "y")
DP = ("x", "c")
ZZ = ("zl", "zh")
YX = ("y", "x")

EPSILON = 1e-06
NEG_FILL = -1e30
F32 = jnp.float32
BF16 = jnp.bfloat16
EXTRA = 8
LIVE = 896


def split_pair(value):
    high = value.astype(BF16)
    return high, (value - high.astype(F32)).astype(BF16)


def dot(a, b):
    return lax.dot_general(a, b, (((1,), (0,)), ((), ())), preferred_element_type=F32)


def dot_nt(a, b):
    return lax.dot_general(a, b, (((1,), (1,)), ((), ())), preferred_element_type=F32)


def dot_tn(a, b):
    return lax.dot_general(a, b, (((0,), (0,)), ((), ())), preferred_element_type=F32)


def places(kk, base, ways, toks):
    per = toks // ways
    row = lax.broadcasted_iota(jnp.int32, (toks, toks), 0)
    turn = row // per + ways - base.astype(jnp.int32)
    turn = jnp.where(turn >= ways, turn - ways, turn)
    return (ways * (row % per) + turn == kk.astype(jnp.int32)).astype(BF16)


def chosen(rank, count):
    at = lax.broadcasted_iota(jnp.int32, (count, rank.shape[1]), 0)
    return (at == rank.astype(jnp.int32)).astype(BF16)


def project_kernel(nx, toks, where, tokens, swapped, rank, gain, gates, *rest):
    weights, out = rest[:-1], rest[-1]
    y, c = where[0], where[1]
    ny = len(weights) // 2
    feat = tokens.shape[-1]
    halves = []
    squares = []
    compact = len(tokens.shape) == 2
    if compact:
        pick = chosen(rank[pl.ds(c, 1), :], tokens.shape[0])
    for source, half in ((tokens, c), (swapped, 1 - c)):
        if compact:
            wide = dot_tn(pick, source[...])
        else:
            wide = source[c].reshape(nx * toks, feat).astype(F32)
        halves.append((wide * gain[pl.ds(half, 1), :]).astype(BF16))
        squares.append(split_pair(wide * wide))
    gate_half = [gates[c], gates[1 - c]]
    ones = jnp.ones((8, feat), BF16)
    extras = []
    for xi in range(nx):
        rows = slice(xi * toks, (xi + 1) * toks)
        both = dot_nt(gate_half[0], halves[0][rows]) + dot_nt(gate_half[1], halves[1][rows])
        square = sum(dot_nt(ones, part[rows]) for pair in squares for part in pair)
        extras.append((both, square))
    for k in range(ny):
        head = lax.rem(y + ny - k, ny)
        done = dot(halves[0], weights[2 * k][:feat]) + dot(halves[1], weights[2 * k + 1][:feat])
        out[head, :, :toks, :] = done.astype(BF16).reshape(nx, toks, done.shape[1])
    out[:, :, toks:, :] = jnp.zeros((ny, nx, EXTRA, out.shape[3]), BF16)
    for xi in range(nx):
        both, square = extras[xi]
        high, low = (p.astype(F32) for p in split_pair(both))
        s_high, s_low = (p.astype(F32) for p in split_pair(square))
        for head in range(ny):
            a, b = 2 * head, 2 * head + 1
            block = jnp.concatenate(
                [
                    high[a : a + 1],
                    low[a : a + 1],
                    high[b : b + 1],
                    low[b : b + 1],
                    s_high[0:1],
                    s_low[0:1],
                    jnp.zeros((2, toks), F32),
                ],
                axis=0,
            )
            out[head, xi, toks:, :toks] = block.astype(BF16)


def cell_kernel(width, span, classed, parts, extras, aux, cell, normer, cell_out, normer_out, stabil_out, gated):
    ways = parts.shape[0] if classed else gated.shape[0]
    toks = gated.shape[2] if classed else gated.shape[2] * ways
    size = cell.shape[1]
    seqs = toks // span
    place = places(aux[0, 3:4, :toks], aux[0, 4:5, :toks], ways, toks)
    if classed:
        per = toks // ways
        wide = parts[:, 0].astype(F32)
        more = extras[:, 0, :, :128].astype(F32)
        for xi in range(1, parts.shape[1]):
            wide = wide + parts[:, xi].astype(F32)
            more = more + extras[:, xi, :, :128].astype(F32)
        high, low = split_pair(wide.reshape(toks, wide.shape[2]))
        total = dot_tn(place, high) + dot_tn(place, low)
        kk = aux[0, 3:4, :toks].astype(jnp.int32)
        at = kk + aux[0, 4:5, :toks].astype(jnp.int32)
        at = at - at // ways * ways
        at = at * 128 + pl.program_id(0) * per + kk // ways
        at = jnp.where(kk < 0, -1, at)
        lane = lax.broadcasted_iota(jnp.int32, (ways * 128, toks), 0)
        move = (lane == at).astype(BF16)
        more = jnp.concatenate([more[way] for way in range(ways)], axis=1)
        extra = jnp.zeros((EXTRA, toks), F32)
        for _ in range(3):
            now = more.astype(BF16)
            extra = extra + dot(now, move)
            more = more - now.astype(F32)
        extra = jnp.concatenate([extra, jnp.zeros((EXTRA, 128 - toks), F32)], axis=1)
    else:
        total = parts[0, 0].astype(F32)
        for xi in range(1, parts.shape[1]):
            total = total + parts[0, xi].astype(F32)
        extra = total[toks:, :128]
    rows = jnp.concatenate([extra, aux[0]], axis=0)
    cols = jnp.transpose(rows)[:toks]
    rows = rows[:, :toks]

    def small(get):
        scale = lax.rsqrt((get(4) + get(5)) / width + EPSILON)
        live = get(9) > 0.5
        gate_in = jnp.where(live, scale * (get(0) + get(1)), NEG_FILL)
        forget = scale * (get(2) + get(3)) + get(10)
        log_forget = jnp.minimum(forget, 0.0) - jnp.log1p(jnp.exp(-jnp.abs(forget)))
        return scale, live, gate_in, jnp.where(live, log_forget, 0.0), get(8)

    _, _, in_row, lf_row, m_row = small(lambda i: rows[i : i + 1])
    scale, live, in_col, lf_col, m_col = small(lambda i: cols[:, i : i + 1])
    at_row = lax.broadcasted_iota(jnp.int32, (toks, toks), 0)
    at_col = lax.broadcasted_iota(jnp.int32, (toks, toks), 1)
    same = (at_row // span) == (at_col // span)
    causal = same & (at_col <= at_row)
    anti = same & (at_row <= at_col)
    c_col = jnp.sum(jnp.where(causal, lf_row, 0.0), axis=1, keepdims=True)
    c_row = jnp.sum(jnp.where(anti, lf_col, 0.0), axis=0, keepdims=True)
    last_col = jnp.sum(jnp.where(same, lf_row, 0.0), axis=1, keepdims=True)
    last_row = jnp.sum(jnp.where(same, lf_col, 0.0), axis=0, keepdims=True)
    weight = jnp.where(causal, c_col - c_row + in_row, NEG_FILL)
    carried = c_col + m_col
    running = jnp.maximum(jnp.max(weight, axis=1, keepdims=True), carried)
    carry = jnp.exp(carried - running)

    def piece(i):
        return (scale * total[:toks, i * size : (i + 1) * size]).astype(BF16)

    query, key_vec, value, outgate = (piece(i) for i in range(4))
    shrink = size**-0.5
    scores = dot_nt(query, key_vec) * shrink * jnp.exp(weight - running)
    s_high, s_low = split_pair(scores)
    carried_out = []
    carried_norm = []
    query_wide = query.astype(F32)
    for r in range(seqs):
        at = slice(r * span, (r + 1) * span)
        high, low = split_pair(cell[r])
        carried_out.append(dot(query[at], high) + dot(query[at], low))
        carried_norm.append(jnp.sum(query_wide[at] * normer[0, r : r + 1], axis=1, keepdims=True))
    numer = dot(s_high, value) + dot(s_low, value) + carry * jnp.concatenate(carried_out, axis=0)
    denom = jnp.sum(scores, axis=1, keepdims=True) + carry * jnp.concatenate(carried_norm, axis=0)
    readout = jnp.where(live, numer / jnp.maximum(jnp.abs(denom), 1.0), 0.0)
    mixed = (readout * jax.nn.sigmoid(outgate.astype(F32))).astype(BF16)
    if not classed:
        mixed = dot(place, mixed).astype(BF16).reshape(ways, toks // ways, size)
    for xi in range(gated.shape[1]):
        if classed:
            gated[0, xi] = mixed
        else:
            gated[:, xi] = mixed

    top_col = jnp.maximum(
        jnp.max(jnp.where(same, last_col - c_row + in_row, NEG_FILL), axis=1, keepdims=True),
        last_col + m_col,
    )
    top_row = jnp.maximum(
        jnp.max(jnp.where(same, last_row - c_col + in_col, NEG_FILL), axis=0, keepdims=True),
        last_row + m_row,
    )
    source = jnp.exp(last_col - c_col + in_col - top_col)
    decay = jnp.exp(last_col + m_col - top_col)
    keyed = (key_vec.astype(F32) * shrink) * source
    k_high, k_low = split_pair(jnp.transpose(keyed))
    token_seq = lax.broadcasted_iota(jnp.int32, (toks, size), 0) // span
    for r in range(seqs):
        at = slice(r * span, (r + 1) * span)
        one = jnp.where(token_seq == r, value.astype(F32), 0.0).astype(BF16)
        fade = decay[r * span : r * span + 1]
        cell_out[r] = fade * cell[r] + (dot(k_high, one) + dot(k_low, one))
        normer_out[0, r : r + 1] = fade * normer[0, r : r + 1] + jnp.sum(
            keyed[at], axis=0, keepdims=True
        )
    stabil_out[0] = jnp.broadcast_to(top_row, (8, toks))


def gather_kernel(where, gated, rank, rank_here, own, *rest):
    weights, out = rest[:-1], rest[-1]
    y = where[0]
    ny = len(weights)
    cores, _, nx, toks, size = gated.shape
    total = dot(chosen(rank_here[0:1, :], out.shape[0]), own[...])
    picks = [chosen(rank[i : i + 1, :], out.shape[0]) for i in range(cores)]
    for k in range(ny):
        head = lax.rem(y + ny - k, ny)
        rows = sum(
            dot(picks[i], gated[i, head].reshape(nx * toks, size)) for i in range(cores)
        ).astype(BF16)
        total = total + dot(rows, weights[k][-size:])
    out[...] = total.astype(BF16)


def mix_kernel(where, gated, *rest):
    weights, out = rest[:-1], rest[-1]
    y = where[0]
    ny = len(weights)
    cores, _, nx, toks, size = gated.shape
    for core in range(cores):
        total = None
        for k in range(ny):
            head = lax.rem(y + ny - k, ny)
            part = dot(gated[core, head].reshape(nx * toks, size), weights[k][-size:])
            total = part if total is None else total + part
        out[core] = total.astype(BF16).reshape(nx, toks, total.shape[1])


def add_kernel(parts, spread):
    total = parts[0].astype(F32)
    for i in range(1, parts.shape[0]):
        total = total + parts[i].astype(F32)
    done = total.astype(BF16)
    for i in range(spread.shape[0]):
        spread[i] = done


def last_kernel(ways, parts, rows, tokens, home, out):
    total = parts[0].astype(F32)
    for i in range(1, parts.shape[0]):
        total = total + parts[i].astype(F32)
    toks = tokens.shape[0]
    place = places(home[0:1, :toks], home[1:2, :toks], ways, toks)
    own = dot_tn(place, rows[...])
    alive = dot_tn(place, jnp.ones(rows.shape, BF16))
    out[...] = jnp.where(alive > 0.5, own + total, tokens[...].astype(F32)).astype(BF16)


def index_kernel(groups, span, where, bias, tops, own, *rest):
    came, (aux, rank, rank_here, home) = rest[:-4], rest[-4:]
    y, x, z = where[0], where[2], where[3]
    nx = len(came)
    quarters, seqs = own.shape
    toks = seqs * span
    lanes = groups * quarters

    def grid(rows, cols):
        return (
            lax.broadcasted_iota(jnp.int32, (rows, cols), 0),
            lax.broadcasted_iota(jnp.int32, (rows, cols), 1),
        )

    def times(mask, value):
        return dot(mask.astype(BF16), value.astype(BF16))

    def spread_seqs(some):
        at = grid(some.shape[0], toks)[1] // span
        return sum(jnp.where(at == r, some[:, r : r + 1], 0.0) for r in range(seqs))

    def numbered(some):
        _, lane = grid(some.shape[0], toks)
        before = sum(
            jnp.where(lane // span > r, some[:, r : r + 1], 0.0) for r in range(seqs - 1)
        )
        slot = lane % span
        live = slot.astype(F32) < spread_seqs(some)
        return jnp.where(live, before + slot.astype(F32), -1.0), live

    def turned(value):
        return value - quarters * jnp.floor(value * (1.0 / quarters))

    def base_of(some):
        row, col = grid(some.shape[0], some.shape[0])
        held = jnp.sum(some, axis=1, keepdims=True)
        earlier = (row // quarters == col // quarters) & (col < row)
        base = times(earlier, jnp.broadcast_to(held, (some.shape[0], 128)))[:, :1]
        return turned(base), held

    mine = own[...].astype(F32)
    kk, live = numbered(mine)
    base, _ = base_of(mine)
    aux[...] = jnp.zeros(aux.shape, F32)
    for layer in range(aux.shape[0]):
        top = spread_seqs(tops[layer])
        for q in range(quarters):
            aux[layer, q, 0:1, :toks] = top[q : q + 1]
            aux[layer, q, 1:2, :toks] = live[q : q + 1].astype(F32)
            aux[layer, q, 2:3, :toks] = jnp.full((1, toks), bias[layer], F32)
            aux[layer, q, 3:4, :toks] = kk[q : q + 1]
            aux[layer, q, 4:5, :toks] = jnp.broadcast_to(base[q : q + 1], (1, toks))

    row, col = grid(lanes, came[0].shape[0])
    everyone = jnp.zeros((lanes, seqs), F32)
    for k in range(nx):
        from_x = lax.rem(x + nx - k, nx)
        cores = groups // nx
        hit = (row // (quarters * cores) == from_x) & (row % (quarters * cores) == col)
        everyone = everyone + times(hit, came[k][...])
    kk_all, _ = numbered(everyone)
    base_all, held_all = base_of(everyone)
    here = grid(lanes, toks)[0] == z * quarters + y
    home[...] = jnp.zeros(home.shape, F32)
    home[0:1] = jnp.sum(jnp.where(here, kk_all, 0.0), axis=0, keepdims=True)
    home[1:2] = jnp.sum(jnp.where(here, base_all, 0.0), axis=0, keepdims=True)

    per = toks // quarters
    turn = turned(y.astype(F32) + quarters - base_all)
    lane = grid(lanes, 128)[1]
    alive = (quarters * lane.astype(F32) + turn < held_all) & (lane < per)
    up, down = grid(128, 128)
    inside = times(alive, (up < down).astype(F32))
    held = jnp.broadcast_to(
        jnp.sum(alive.astype(F32), axis=1, keepdims=True), (lanes, 128)
    )
    up, down = grid(lanes, lanes)
    order = jnp.where(alive, inside + times(down < up, held), -1.0)
    ranks = jnp.zeros((groups, toks), F32)
    for q in range(quarters):
        up, down = grid(groups, lanes)
        picked = times(down == up * quarters + q, order)
        up, down = grid(128, toks)
        ranks = ranks + dot(picked.astype(BF16), (down == up + q * per).astype(BF16)) * (
            grid(groups, toks)[1] // per == q
        ).astype(F32)
    at = grid(groups, toks)[0] == z
    rank_here[...] = jnp.broadcast_to(
        jnp.sum(jnp.where(at, ranks, 0.0), axis=0, keepdims=True), rank_here.shape
    )
    cores, wide = rank.shape
    for core in range(cores):
        total = jnp.zeros((8, wide), F32)
        for xi in range(nx):
            one = jnp.broadcast_to(ranks[cores * xi + core : cores * xi + core + 1], (8, toks))
            up, down = grid(toks, wide)
            total = total + dot(one.astype(BF16), (down == up + xi * toks).astype(BF16))
        rank[core : core + 1] = total[:1]


def pack_kernel(query, key_vec, value, outgate, last, joined, *spread):
    size = query.shape[2]
    feat = query.shape[1]
    for i, source in enumerate((query, key_vec, value, outgate)):
        joined[:feat, i * size : (i + 1) * size] = source[0]
    for copies in spread:
        for i in range(copies.shape[0]):
            copies[i] = last[...]
    if not spread:
        joined[feat:] = last[0]


SMEM_SPEC = pl.BlockSpec(memory_space=pltpu.SMEM)
VMEM_SPEC = pl.BlockSpec(memory_space=pltpu.VMEM)
HBM_SPEC = pl.BlockSpec(memory_space=pltpu.HBM)


def per_device(
    tokens,
    lengths,
    norm_gain,
    query_weight,
    key_weight,
    value_weight,
    outgate_weight,
    input_gate_weight,
    forget_gate_weight,
    forget_bias,
    out_weight,
    cell_state,
    norm_state,
    max_state,
):
    seq_here, span, feat = tokens.shape
    layers, local_seqs, _, size, _ = cell_state.shape
    ny, nx, nc, nz = (lax.axis_size(a) for a in ("y", "x", "c", ZZ))
    toks = seq_here * span
    width = feat * nx * nc
    y, x, c = (lax.axis_index(a) for a in ("y", "x", "c"))
    z = lax.axis_index("zh") * lax.axis_size("zl") + lax.axis_index("zl")
    where = jnp.stack([y, c, x, z]).astype(jnp.int32)
    quarters = local_seqs // seq_here

    def shifted(array, step):
        return lax.ppermute(array, "y", [(i, (i + step) % ny) for i in range(ny)])

    def swapped(array):
        return lax.ppermute(array, "c", [(i, (i + 1) % nc) for i in range(nc)])

    def exchanged(rows):
        height = toks // ny
        came = [
            shifted(lax.dynamic_slice(rows, ((y + k) % ny * height, 0), (height, feat)), k)
            if k
            else lax.dynamic_slice(rows, (y * height, 0), (height, feat))
            for k in range(ny)
        ]
        came = jnp.concatenate(came, axis=0)
        return jnp.concatenate(
            [
                lax.dynamic_slice(came, ((y + ny - q) % ny * height, 0), (height, feat))
                for q in range(ny)
            ],
            axis=0,
        )

    gains = lax.all_gather(norm_gain, "c", axis=0)
    pair = swapped(lengths)
    pair = jnp.where(c == 0, jnp.stack([lengths, pair]), jnp.stack([pair, lengths]))
    turned = [pair] + [
        lax.ppermute(pair, "x", [(i, (i + k) % nx) for i in range(nx)]) for k in range(1, nx)
    ]
    per = toks // ny
    live = [t.reshape(nc * quarters, seq_here) for t in turned]
    auxes, rank, rank_here, home = pl.pallas_call(
        lambda *refs: index_kernel(nx * nc, span, *refs),
        out_shape=(
            jax.ShapeDtypeStruct((layers, quarters, 8, 128), F32),
            jax.ShapeDtypeStruct((nc, nx * toks), F32),
            jax.ShapeDtypeStruct((8, toks), F32),
            jax.ShapeDtypeStruct((8, toks), F32),
        ),
        in_specs=[SMEM_SPEC] * 2 + [VMEM_SPEC] * (2 + nx),
        out_specs=(VMEM_SPEC,) * 4,
        compiler_params=pltpu.CompilerParams(vmem_limit_bytes=4 << 20),
        name="index",
    )(
        where,
        forget_bias.reshape(layers),
        max_state.reshape(layers, quarters, seq_here),
        lengths.reshape(quarters, seq_here),
        *live,
    )
    compact = -(-(LIVE // ny + nz) // (16 * nz)) * 16 * nz

    def gates_of(layer):
        cut = [
            lax.dynamic_slice(w[layer], (x * nc * feat, z * ny), (nc * feat, ny))
            for w in (input_gate_weight, forget_gate_weight)
        ]
        both = jnp.stack(cut, axis=2).reshape(nc, feat, 2 * ny)
        return jnp.transpose(both, (0, 2, 1))

    projections = (query_weight, key_weight, value_weight, outgate_weight)
    current = tokens.reshape(toks, feat)

    def pack(layer, last, last_spec, out_shape):
        whole = [pl.BlockSpec(o.shape, lambda i, n=len(o.shape): (0,) * n) for o in out_shape]
        return pl.pallas_call(
            pack_kernel,
            grid=(1,),
            out_shape=out_shape,
            in_specs=[pl.BlockSpec((1, feat, size), lambda i: (layer, 0, 0))] * 4 + [last_spec],
            out_specs=whole,
            compiler_params=pltpu.CompilerParams(vmem_limit_bytes=60 << 20),
        )(*projections, last)

    joined, spread = pack(
        0,
        current,
        pl.BlockSpec((toks, feat), lambda i: (0, 0)),
        [
            jax.ShapeDtypeStruct((feat, 4 * size), BF16),
            jax.ShapeDtypeStruct((nz, toks, feat), BF16),
        ],
    )
    spread = spread.reshape(nz * toks, feat)
    moved = [joined] + [shifted(joined, k) for k in range(1, ny)]
    weights = []
    for w in moved:
        weights += [w, swapped(w)]
    states = []
    for layer in range(layers):
        arrived = lax.all_to_all(spread, ZZ, 0, 0, tiled=True)
        if layer == 0:
            (packed,) = pack(
                1,
                out_weight,
                pl.BlockSpec((1, size, feat), lambda i: (1, 0, 0)),
                [jax.ShapeDtypeStruct((feat + size, 4 * size), BF16)],
            )
            gates = [gates_of(n) for n in range(layers)]
            gains = [gains[:, n] for n in range(layers)]
            (arrived, gates, gains, packed) = lax.optimization_barrier(
                (arrived, gates, gains, packed)
            )
            rows = dot(places(home[0:1], home[1:2], ny, toks), current).astype(BF16)
        other = swapped(arrived)
        if layer:
            rows = dot_tn(chosen(rank_here[0:1], compact), arrived).astype(BF16)
        if layer == 0:
            other = other.reshape(nc, nx, toks, feat)
            arrived = arrived.reshape(nc, nx, toks, feat)
        parts = pl.pallas_call(
            lambda *refs: project_kernel(nx, toks, *refs),
            out_shape=jax.ShapeDtypeStruct((ny, nx, toks + EXTRA, 4 * size), BF16),
            in_specs=[SMEM_SPEC] + [VMEM_SPEC] * (5 + 2 * ny),
            out_specs=VMEM_SPEC,
            compiler_params=pltpu.CompilerParams(vmem_limit_bytes=60 << 20),
        )(where, arrived, other, rank if layer else gains[layer], gains[layer], gates[layer], *weights)
        rows = exchanged(rows)
        summed = lax.all_to_all(
            parts.reshape(ny * nx * (toks + EXTRA), 4 * size), YX, 0, 0, tiled=True
        ).reshape(ny, nx, toks + EXTRA, 4 * size)
        if layer == 0:
            rows, summed = lax.optimization_barrier((rows, summed))
        if layer == 0:
            outs = [out_weight[0]] + [shifted(out_weight[0], k) for k in range(1, ny)]
            near = {k: shifted(packed, k) for k in (1, ny - 1)}
        first = layer * quarters
        state_specs = (
            pl.BlockSpec((seq_here, size, size), lambda i: (first + i, 0, 0)),
            pl.BlockSpec((1, seq_here, size), lambda i: (first + i, 0, 0)),
            pl.BlockSpec((1, 8, toks), lambda i: (first + i, 0, 0)),
        )
        kept = [HBM_SPEC] * len(states)
        part_block = (1, nx, toks + EXTRA, 4 * size)
        part_spec = pl.BlockSpec(part_block, lambda i: (i, 0, 0, 0))
        extra_at = (0, 0, 0, 0)
        send_spec = pl.BlockSpec((ny, nx, per, size), lambda i: (0, 0, i, 0))
        if layer:
            part_spec = pl.BlockSpec((ny, nx, per, 4 * size), lambda i: (0, 0, i, 0))
            extra_at = (0, 0, toks // EXTRA, 0)
            send_spec = pl.BlockSpec((1, nx, toks, size), lambda i: (i, 0, 0, 0))
        *states, gated = pl.pallas_call(
            lambda *refs: cell_kernel(
                width, span, layer > 0, *refs[:5], *refs[5 + len(kept) :]
            ),
            grid=(quarters,),
            out_shape=(
                jax.ShapeDtypeStruct((layers * local_seqs, size, size), F32),
                jax.ShapeDtypeStruct((layers * quarters, seq_here, size), F32),
                jax.ShapeDtypeStruct((layers * quarters, 8, toks), F32),
                jax.ShapeDtypeStruct((quarters, nx, toks, size), BF16),
            ),
            in_specs=[
                part_spec,
                pl.BlockSpec((ny, nx, EXTRA, 4 * size), lambda i: extra_at),
                pl.BlockSpec((1, 8, 128), lambda i: (first + i, 0, 0)),
                *state_specs[:2],
                *kept,
            ],
            out_specs=(
                *state_specs,
                send_spec,
            ),
            input_output_aliases={5 + n: n for n in range(len(kept))},
            compiler_params=pltpu.CompilerParams(vmem_limit_bytes=10 << 20),
        )(
            summed,
            summed,
            auxes.reshape(layers * quarters, 8, 128),
            cell_state.reshape(layers * local_seqs, size, size),
            norm_state.reshape(layers * quarters, seq_here, size),
            *states,
        )
        heads = lax.all_to_all(
            gated.reshape(quarters * nx * toks, size), YX, 0, 0, tiled=True
        ).reshape(ny, nx, toks, size)
        if layer + 1 < layers:
            late, heads = lax.optimization_barrier((packed, heads))
            far = {k: shifted(late, k) for k in range(2, ny - 1)}
            moved = [packed] + [(near | far)[k] for k in range(1, ny)]
            weights = []
            for w in moved:
                weights += [w, swapped(w)]
            next_outs = moved
        everyone = lax.all_gather(heads, "c", axis=0)
        if layer + 1 < layers:
            mixed = pl.pallas_call(
                gather_kernel,
                out_shape=jax.ShapeDtypeStruct((compact, feat), BF16),
                in_specs=[SMEM_SPEC] + [VMEM_SPEC] * (4 + ny),
                out_specs=VMEM_SPEC,
                compiler_params=pltpu.CompilerParams(vmem_limit_bytes=60 << 20),
            )(where, everyone, rank, rank_here, rows, *outs)
            added = lax.all_to_all(mixed, ZZ, 0, 0, tiled=True)
            spread = pl.pallas_call(
                add_kernel,
                out_shape=jax.ShapeDtypeStruct((nz, compact // nz, feat), BF16),
                in_specs=[VMEM_SPEC],
                out_specs=VMEM_SPEC,
                compiler_params=pltpu.CompilerParams(vmem_limit_bytes=8 << 20),
            )(added.reshape(nz, compact // nz, feat))
            spread = spread.reshape(compact, feat)
            outs = next_outs
            continue
        mixed = pl.pallas_call(
            mix_kernel,
            out_shape=jax.ShapeDtypeStruct((nc, nx, toks, feat), BF16),
            in_specs=[SMEM_SPEC] + [VMEM_SPEC] * (1 + ny),
            out_specs=VMEM_SPEC,
            compiler_params=pltpu.CompilerParams(vmem_limit_bytes=8 << 20),
        )(where, everyone, *outs)
        added = lax.all_to_all(mixed.reshape(nz * toks, feat), ZZ, 0, 0, tiled=True)
        current = pl.pallas_call(
            lambda *refs: last_kernel(ny, *refs),
            out_shape=jax.ShapeDtypeStruct((toks, feat), BF16),
            in_specs=[VMEM_SPEC] * 4,
            out_specs=VMEM_SPEC,
            compiler_params=pltpu.CompilerParams(vmem_limit_bytes=8 << 20),
        )(added.reshape(nz, toks, feat), rows, current, home)
    cell_next, normer_next, top = states
    return (
        current.reshape(seq_here, span, feat),
        cell_next.reshape(cell_state.shape),
        normer_next.reshape(norm_state.shape),
        top[:, 0, ::span].reshape(max_state.shape),
    )


def solution(mesh):
    finer = Mesh(mesh.devices.reshape(4, 2, 4, 4, 2), ("zh", "zl", "y", "x", "c"))
    placed = (
        P(TP, None, DP),
        P(DP),
        P(None, DP),
        P(None, DP, TP),
        P(None, DP, TP),
        P(None, DP, TP),
        P(None, DP, TP),
        P(),
        P(),
        P(None, TP),
        P(None, TP, DP),
        P(None, DP, TP, None, None),
        P(None, DP, TP, None),
        P(None, DP, TP),
    )

    return jax.shard_map(
        per_device,
        mesh=finer,
        in_specs=placed,
        out_specs=(
            P(TP, None, DP),
            P(None, DP, TP, None, None),
            P(None, DP, TP, None),
            P(None, DP, TP),
        ),
        check_vma=False,
    )
```
